32 devices in a mesh: sp: 8 (over z, core), tp: 4 (over y, x).
Axes of the slice: x: 2, y: 2, z: 4, core: 2. Of those that a mesh axis runs over, the one named last changes fastest.
Arguments:
- pool_in: bfloat16 [512, 3072], P('tp', 'sp'), may hold values from -8 to 8
- doc_ids: int32 [3072], P('sp'), may hold values from 0 to 3, never falling along the last dimension, each value on 1 to 1536 neighbouring positions
- pool_map: bfloat16 [8, 64, 64], replicated, may hold values from -0.75 to 0.75
- pool_scale: float32 [512], replicated, may hold values from 0.1 to 1.9
- w_out: bfloat16 [512, 2048], P(None, 'tp'), may hold values from -0.25 to 0.25
- gate_logit: bfloat16 [3072, 2048], P('sp', 'tp'), may hold values from -8 to 8
- residual: bfloat16 [3072, 2048], P('sp', 'tp'), may hold values from -4 to 4
- first_gain: float32 [2048], P('tp'), may hold values from 0.1 to 1.9
- first_bias: float32 [2048], P('tp'), may hold values from -1.5 to 1.5
- routes: int32 [3072, 2], P('sp'), may hold values from 0 to 7, all different within a row; in each aligned block of 384 rows (0 to 383, 384 to 767, ...) at most 192 rows name the same one
- route_weight: float32 [3072, 2], P('sp'), may hold values from 0.25 to 1
- w_gate: bfloat16 [8, 2048, 1024], P('sp', None, 'tp'), may hold values from -0.125 to 0.125
- w_up: bfloat16 [8, 2048, 1024], P('sp', None, 'tp'), may hold values from -0.125 to 0.125
- w_down: bfloat16 [8, 1024, 2048], P('sp', None, 'tp'), may hold values from -0.375 to 0.375
- second_gain: float32 [2048], P('tp'), may hold values from 0.1 to 1.9
- second_bias: float32 [2048], P('tp'), may hold values from -1.5 to 1.5
Outputs:
- layer_out: bfloat16 [3072, 2048], P('sp', 'tp')
The draws below stay inside these ranges and needn't reach their ends.
Inputs may be any that keep to these rules, and one draw needn't show every extreme that they name: `doc_ids`: never falling; each document spans 1 to 1536 positions. `routes`: each row names 2 different experts; in each aligned block of 384 rows (the rows of one index of sp) no expert is named by more than 192 rows, a bound that some block reaches.
All inputs are finite; a program needn't handle non-finite values.
Results may differ from the reference program's by a relative error of at most 0.008.
Values may be sent and summed in bfloat16 or wider, within the bound.
A program may use at most 64 MiB of HBM per device.

```python
import math
import jax
import jax.numpy as jnp
import numpy as np
from jax import lax

D = 2048
MIX_W = 512
GROUP_W = 64
GROUPS = 8
DE = 1024
TOPK = 2
TOK_DEV = 384
TOKENS = 3072
EXPERTS = 8
CAP = 192
DOCS = 4
DOC_MOST = 1536
N_SP = 8


def draw_pool_in(key, part):
    walk_key, rough_key = jax.random.split(jax.random.fold_in(key, 7))
    blocks = TOKENS // 16
    drift_walk = jnp.cumsum(jax.random.normal(walk_key, (MIX_W, blocks), jnp.float32), axis=1)
    drift_walk = drift_walk / jnp.sqrt(jnp.float32(blocks))
    smooth = jnp.repeat(drift_walk, 16, axis=1)
    rough_part = jax.random.normal(rough_key, (MIX_W, TOKENS), jnp.float32)
    return jnp.clip(0.8 * rough_part + smooth, -8.0, 8.0).astype(jnp.bfloat16)


def level_of(own_key, shape, shards, least, top_value):
    loudness = 1.0
    for dim, blocks in shards:
        steps = jax.random.uniform(jax.random.fold_in(jax.random.fold_in(own_key, 6), dim), (blocks,), jnp.float32, least / len(shards), top_value / len(shards))
        loudness = loudness * jnp.repeat(jnp.exp(steps), shape[dim] // blocks).reshape((-1,) + (1,) * (len(shape) - 1 - dim))
    return loudness


def length_profile(amount, total, limit, lean):
    portions = [(1 << 20) // math.isqrt(standing ** lean) + 1 for standing in range(2, amount + 1)]
    spare, holding = total - limit - (amount - 1), [1] * (amount - 1)
    while spare > 0:
        candidates = [i for i in range(amount - 1) if holding[i] < limit]
        whole, left = sum([portions[i] for i in candidates]), spare
        for i in candidates:
            addition = min(limit - holding[i], max(1, left * portions[i] // whole), spare)
            holding[i] = holding[i] + addition
            spare = spare - addition
    return np.array([limit] + holding)


def uneven(rng, number_of, total, bound, lean):
    if number_of == 2:
        one = jax.random.randint(rng, (), max(1, total - bound), min(bound, total - 1) + 1)
        return jnp.stack([one, total - one])
    lengths = jnp.asarray(length_profile(number_of, total, bound, lean), jnp.int32)
    twos = (number_of - 1) // 2
    giver, receiver = lengths[1:1 + 2 * twos:2], lengths[2:2 + 2 * twos:2]
    room = jnp.minimum(giver - 1, bound - receiver)
    passed = jax.random.randint(jax.random.fold_in(rng, 1), (twos,), 0, 1 << 20) % (room + 1)
    lengths = lengths.at[1:1 + 2 * twos:2].set(giver - passed).at[2:2 + 2 * twos:2].set(receiver + passed)
    return lengths[jax.random.permutation(jax.random.fold_in(rng, 2), number_of)]


def routed_block(stream_key, own, number, rows, amount, top, most, slope):
    order = jax.random.permutation(stream_key, amount)
    crowded, ordinary = portions_of(amount, rows * top, most, slope, True), portions_of(amount, rows * top, most, slope, False)
    places = jnp.arange(amount)

    def named(lengths, rotation):
        used = int((lengths > 0).sum())
        fixed = max(1, used // 4)
        shifted = fixed + (places - fixed + rotation * (used - fixed)) % max(1, amount - fixed)
        return jnp.zeros((amount,), jnp.int32).at[order[jnp.where(places < fixed, places, shifted)]].set(jnp.asarray(lengths, jnp.int32))

    lengths = jnp.where(number % 4 == 0, named(crowded, number // 4), named(ordinary, number - number // 4 - 1))
    mixed = jax.random.permutation(jax.random.fold_in(own, 3), amount)
    donor, receiver = mixed[0:amount // 2 * 2:2], mixed[1:amount // 2 * 2:2]
    slack = jnp.minimum(lengths[donor] - 1, most - lengths[receiver]) // 2
    slack = jnp.where((donor == order[0]) | (receiver == order[0]) | (lengths[receiver] == 0), 0, jnp.maximum(slack, 0))
    shifted = jax.random.randint(jax.random.fold_in(own, 4), (amount // 2,), 0, 1 << 20) % (slack + 1)
    lengths = lengths.at[donor].add(-shifted).at[receiver].add(shifted)
    labels = jnp.searchsorted(jnp.cumsum(lengths), jnp.arange(rows * top), side="right").astype(jnp.int32)
    grid = labels.reshape(top, rows).T
    grid = grid[jax.random.permutation(jax.random.fold_in(own, 1), rows)]
    rotation = jax.random.randint(jax.random.fold_in(own, 2), (rows, 1), 0, top)
    return jnp.take_along_axis(grid, (jnp.arange(top)[None, :] + rotation) % top, axis=1)


def portions_of(amount, total, limit, slope, full):
    loads = [(1 << 20) // math.isqrt(rank ** slope) + 1 for rank in range(1, amount + 1)]
    largest = limit if full else min(limit, max(-(-total // amount), total * loads[0] // sum(loads)))
    least = 1 if total - largest >= amount - 1 else 0
    holding, spare = [largest] + [least] * (amount - 1), total - largest - least * (amount - 1)
    while spare > 0:
        candidates = [i for i in range(1, amount) if holding[i] < largest] or [i for i in range(1, amount) if holding[i] < limit]
        pool, left = sum([loads[i] for i in candidates]), spare
        for i in candidates:
            more = min(limit - holding[i], max(1, left * loads[i] // pool), spare)
            holding[i] = holding[i] + more
            spare = spare - more
    return np.array(holding)


def gaussian(rng, extent, deviation, limit, cuts=(), held_as=jnp.bfloat16):
    loudness = level_of(rng, extent, cuts, -0.22, 0.18) if cuts else 1.0
    entries = jax.random.normal(rng, extent, jnp.float32) * deviation * loudness
    return jnp.minimum(jnp.maximum(entries, -limit), limit).astype(held_as)


def setup_inputs(seed: int = 0) -> dict:
    arg_keys = jax.random.split(jax.random.key(seed), 17)
    pool_in = draw_pool_in(jax.random.fold_in(arg_keys[16], 71), 0)
    doc_ids = jnp.searchsorted(jnp.cumsum(uneven(arg_keys[1], DOCS, TOKENS, DOC_MOST, 1)), jnp.arange(TOKENS), side="right").astype(jnp.int32)
    pool_map = gaussian(arg_keys[2], (GROUPS, GROUP_W, GROUP_W), GROUP_W ** -0.5, 0.75)
    pool_scale = jnp.clip(1.0 + 0.18 * jax.random.normal(arg_keys[3], (MIX_W,), jnp.float32), 0.1, 1.9)
    w_out = gaussian(arg_keys[4], (MIX_W, D), MIX_W ** -0.5, 0.25, ((1, 4),))
    gate_logit = gaussian(arg_keys[5], (TOKENS, D), 1.5, 8.0, ((0, 8), (1, 4)))
    residual = gaussian(arg_keys[6], (TOKENS, D), 0.6, 4.0, ((0, 8), (1, 4)))
    first_gain = jnp.clip(1.0 + 0.18 * jax.random.normal(arg_keys[7], (D,), jnp.float32), 0.1, 1.9)
    first_bias = gaussian(arg_keys[8], (D,), 0.3, 1.5, ((0, 4),), jnp.float32)
    routes_keys = jax.random.split(jax.random.fold_in(arg_keys[9], 1), TOKENS // TOK_DEV)
    routes_turns = jax.random.permutation(jax.random.fold_in(arg_keys[9], 3), TOKENS // TOK_DEV)
    routes = jax.vmap(lambda own, number: routed_block(jax.random.fold_in(arg_keys[9], 2), own, number, TOK_DEV, EXPERTS, TOPK, CAP, 1))(routes_keys, routes_turns).reshape((TOKENS, TOPK))
    route_weight = jnp.clip(0.25 + 0.75 * jax.random.uniform(arg_keys[10], (TOKENS, TOPK), jnp.float32) ** level_of(arg_keys[10], (TOKENS, TOPK), ((0, 8),), -0.2, 0.2), 0.25, 1.0)
    w_gate = gaussian(arg_keys[11], (EXPERTS, D, DE), D ** -0.5, 0.125, ((0, 8), (2, 4)))
    w_up = gaussian(arg_keys[12], (EXPERTS, D, DE), D ** -0.5, 0.125, ((0, 8), (2, 4)))
    w_down = gaussian(arg_keys[13], (EXPERTS, DE, D), (DE // 4) ** -0.5, 0.375, ((0, 8), (2, 4)))
    second_gain = jnp.clip(1.0 + 0.18 * jax.random.normal(arg_keys[14], (D,), jnp.float32), 0.1, 1.9)
    second_bias = gaussian(arg_keys[15], (D,), 0.3, 1.5, ((0, 4),), jnp.float32)
    return dict(pool_in=pool_in, doc_ids=doc_ids, pool_map=pool_map, pool_scale=pool_scale, w_out=w_out, gate_logit=gate_logit, residual=residual, first_gain=first_gain, first_bias=first_bias, routes=routes, route_weight=route_weight, w_gate=w_gate, w_up=w_up, w_down=w_down, second_gain=second_gain, second_bias=second_bias)


EPS = 1e-05
ALPHA = 8.0 ** 0.25

def layer_norm(row_data, gain_vec, bias_vec):
    row_mean = lax.optimization_barrier(jnp.mean(row_data, axis=1, keepdims=True))
    row_var = lax.optimization_barrier(jnp.mean(row_data * row_data, axis=1, keepdims=True)) - row_mean * row_mean
    return (row_data - row_mean) * lax.rsqrt(row_var + EPS) * gain_vec + bias_vec

def pool_scales(pool_in, doc_ids):
    values = pool_in.astype(jnp.float32)
    length = values.shape[1]
    opening = jnp.concatenate([jnp.ones((1,), bool), doc_ids[1:] != doc_ids[:-1]])
    places = jnp.arange(length, dtype=jnp.int32)
    doc_start = lax.cummax(jnp.where(opening, places, 0), axis=0)
    prefix = jnp.concatenate([jnp.zeros((MIX_W, 1), jnp.float32), jnp.cumsum(values, axis=1)], axis=1)
    upper_at = places + 1
    group_id = jnp.arange(MIX_W, dtype=jnp.int32) // GROUP_W
    doc_mask = (group_id % 2 == 1)[:, None]
    window = jnp.left_shift(2, group_id // 2 % 4)[:, None]
    lower_at = jnp.where(doc_mask, doc_start[None, :], jnp.maximum(upper_at[None, :] - window, doc_start[None, :]))
    lower_at = lower_at.astype(jnp.int32)
    window_sum = prefix[:, 1:] - jnp.take_along_axis(prefix, lower_at, axis=1)
    counted = (upper_at[None, :] - lower_at).astype(jnp.float32)
    return (window_sum / counted - values).astype(jnp.bfloat16)

def reference(pool_in, doc_ids, pool_map, pool_scale, w_out, gate_logit, residual, first_gain, first_bias, routes, route_weight, w_gate, w_up, w_down, second_gain, second_bias):
    pooled = pool_scales(pool_in, doc_ids)
    grouped = jnp.einsum('gct,gcd->tgd', pooled.reshape(GROUPS, GROUP_W, TOKENS).astype(jnp.float32), pool_map.astype(jnp.float32))
    mapped = (grouped.reshape(TOKENS, MIX_W) * pool_scale).astype(jnp.bfloat16)
    mixer_out = jnp.dot(mapped, w_out, preferred_element_type=jnp.float32) * jax.nn.sigmoid(gate_logit.astype(jnp.float32))
    normed = layer_norm(ALPHA * residual.astype(jnp.float32) + mixer_out, first_gain, first_bias).astype(jnp.bfloat16)
    flat_routes = routes.reshape(-1).astype(jnp.int32)
    one_hot = (flat_routes[:, None] == jnp.arange(EXPERTS, dtype=jnp.int32)[None, :]).astype(jnp.int32)
    slot_rank = lax.optimization_barrier(jnp.sum((jnp.cumsum(one_hot, axis=0, dtype=jnp.int32) - 1) * one_hot, axis=1)).astype(jnp.int32)
    rows_most = N_SP * CAP
    token_of = jnp.arange(TOKENS * TOPK, dtype=jnp.int32) // TOPK
    flat_weight = route_weight.reshape(-1)

    def one_expert(running, expert):
        slot_ids = jnp.where(flat_routes == expert, slot_rank, rows_most).astype(jnp.int32)
        picked = jnp.zeros((rows_most,), jnp.int32).at[slot_ids].set(token_of, mode='drop')
        slot_weight = jnp.zeros((rows_most,), jnp.float32).at[slot_ids].set(flat_weight, mode='drop')
        inputs = normed[picked]
        gate_part = jnp.dot(inputs, w_gate[expert], preferred_element_type=jnp.float32)
        up_part = jnp.dot(inputs, w_up[expert], preferred_element_type=jnp.float32)
        hidden = (jax.nn.silu(gate_part) * up_part).astype(jnp.bfloat16)
        result = jnp.dot(hidden, w_down[expert], preferred_element_type=jnp.float32).astype(jnp.bfloat16)
        return (running.at[picked].add(slot_weight[:, None] * result.astype(jnp.float32)), None)
    moe_sum, _ = lax.scan(one_expert, jnp.zeros((TOKENS, D), jnp.float32), jnp.arange(EXPERTS, dtype=jnp.int32))
    return layer_norm(ALPHA * normed.astype(jnp.float32) + moe_sum, second_gain, second_bias).astype(jnp.bfloat16)
```

```python
import functools

import jax
import jax.numpy as jnp
from jax import lax
from jax.experimental import pallas as pl
from jax.experimental.pallas import tpu as pltpu
from jax.sharding import PartitionSpec as P

GROUP_W = 64


EPS = 1e-05
ALPHA = 8.0**0.25
halo_len = 16


def shifted(shard, axis, by):
    size = lax.axis_size(axis)
    pairs = [(i, i + by) for i in range(size) if 0 <= i + by < size]
    return lax.ppermute(shard, axis, pairs)


def entering(shard, axis, combine, identity):
    size, place = (lax.axis_size(axis), lax.axis_index(axis))
    everything = jax.tree.map(lambda part: lax.all_gather(part, axis), shard)
    start = jax.tree.map(
        lambda part, zero: jnp.broadcast_to(jnp.asarray(zero, part.dtype), part.shape),
        shard,
        identity,
    )

    def turn(k, before):
        reached = k < place
        new = combine(before, jax.tree.map(lambda part: part[k], everything))
        return jax.tree.map(lambda a, b: jnp.where(reached, a, b), new, before)

    return lax.fori_loop(0, size, turn, start)


def carry_join(earlier, later):
    keeping = 1.0 - later[2]
    return (
        later[0] + keeping * earlier[0],
        later[1] + keeping * earlier[1],
        jnp.maximum(earlier[2], later[2]),
    )


def apply_norm(row_data, totals, gain_vec, bias_vec, features):
    row_mean = totals[0][:, None] / features
    row_var = totals[1][:, None] / features - row_mean * row_mean
    return (row_data - row_mean) * lax.rsqrt(row_var + EPS) * gain_vec + bias_vec


def pool_scales(pool_in, doc_ids):
    channels_dev, positions = pool_in.shape
    edge_block = jnp.concatenate(
        [
            pool_in[:, positions - halo_len :],
            doc_ids[None, positions - halo_len :].astype(jnp.bfloat16),
        ],
        axis=0,
    )
    previous = shifted(edge_block, "sp", 1)
    prior_ids = jnp.where(
        lax.axis_index("sp") == 0, -1.0, previous[channels_dev].astype(jnp.float32)
    )
    ids_ext = jnp.concatenate([prior_ids, doc_ids.astype(jnp.float32)])
    inputs_ext = jnp.concatenate([previous[:channels_dev], pool_in], axis=1).astype(jnp.float32)
    length = positions + halo_len
    opening = jnp.concatenate([jnp.zeros((1,), bool), ids_ext[1:] != ids_ext[:-1]])
    places = jnp.arange(length, dtype=jnp.int32)
    doc_start = lax.cummax(jnp.where(opening, places, 0), axis=0)
    prefix = jnp.concatenate(
        [jnp.zeros((channels_dev, 1), jnp.float32), jnp.cumsum(inputs_ext, axis=1)], axis=1
    )
    start_here = doc_start[halo_len:]
    upper_at = places[halo_len:] + 1
    at_start = jnp.take(prefix, start_here, axis=1)
    current = prefix[:, halo_len + 1 :]
    group_id = (
        lax.axis_index("tp") * channels_dev + jnp.arange(channels_dev, dtype=jnp.int32)
    ) // GROUP_W
    doc_mask = (group_id % 2 == 1)[:, None]
    window = jnp.left_shift(2, group_id // 2 % 4)[:, None]
    lagged = jnp.zeros((channels_dev, positions), jnp.float32)
    for octave in range(4):
        window_len = 2 << octave
        begin = halo_len + 1 - window_len
        lagged = lagged + jnp.where(window == window_len, prefix[:, begin : begin + positions], 0.0)
    lower_at = jnp.maximum(upper_at[None, :] - window, start_here[None, :])
    win_sum = current - jnp.where(
        start_here[None, :] > upper_at[None, :] - window, at_start, lagged
    )
    win_count = (upper_at[None, :] - lower_at).astype(jnp.float32)
    opened = start_here >= halo_len
    local_sum = current - jnp.where(opened[None, :], at_start, prefix[:, halo_len : halo_len + 1])
    local_count = (upper_at - jnp.maximum(start_here, halo_len)).astype(jnp.float32)
    last_start = doc_start[length - 1]
    last_base = jnp.where(
        last_start >= halo_len,
        lax.dynamic_slice_in_dim(prefix, last_start, 1, 1)[:, 0],
        prefix[:, halo_len],
    )
    summary = (
        prefix[:, length] - last_base,
        (length - jnp.maximum(last_start, halo_len)).astype(jnp.float32),
        (last_start >= halo_len).astype(jnp.float32),
    )
    nothing = (jnp.zeros((channels_dev,), jnp.float32), jnp.float32(0.0), jnp.float32(0.0))
    carried = entering(summary, "sp", carry_join, nothing)
    doc_sum = local_sum + jnp.where(opened[None, :], 0.0, carried[0][:, None])
    doc_count = local_count + jnp.where(opened, 0.0, carried[1])
    pooled = (
        jnp.where(doc_mask, doc_sum / doc_count[None, :], win_sum / win_count)
        - inputs_ext[:, halo_len:]
    )
    return pooled.astype(jnp.bfloat16)


def general_body(
    pool_in,
    doc_ids,
    pool_map,
    pool_scale,
    w_out,
    gate_logit,
    residual,
    first_gain,
    first_bias,
    routes,
    route_weight,
    w_gate,
    w_up,
    w_down,
    second_gain,
    second_bias,
):
    pooled = pool_scales(pool_in, doc_ids)
    positions = pool_in.shape[1]
    features = residual.shape[1] * lax.axis_size("tp")
    gathered = lax.all_gather(pooled, "tp", axis=0, tiled=True)
    group_count = gathered.shape[0] // GROUP_W
    grouped = jnp.einsum(
        "gct,gcd->tgd",
        gathered.reshape(group_count, GROUP_W, positions),
        pool_map,
        preferred_element_type=jnp.float32,
    )
    mapped = (grouped.reshape(positions, group_count * GROUP_W) * pool_scale).astype(jnp.bfloat16)
    mixer_out = jnp.dot(mapped, w_out, preferred_element_type=jnp.float32) * jax.nn.sigmoid(
        gate_logit.astype(jnp.float32)
    )
    mixed_rows = ALPHA * residual.astype(jnp.float32) + mixer_out
    first_totals = lax.psum(
        (jnp.sum(mixed_rows, axis=1), jnp.sum(mixed_rows * mixed_rows, axis=1)), "tp"
    )
    normed = apply_norm(mixed_rows, first_totals, first_gain, first_bias, features).astype(
        jnp.bfloat16
    )
    experts = lax.axis_size("sp")
    pairs = routes.shape[1]
    slots_per = 2 * positions * pairs // experts
    flat_routes = routes.reshape(-1)
    one_hot = (flat_routes[:, None] == jnp.arange(experts, dtype=jnp.int32)[None, :]).astype(
        jnp.int32
    )
    slot_rank = jnp.sum((jnp.cumsum(one_hot, axis=0, dtype=jnp.int32) - 1) * one_hot, axis=1)
    slot_ids = flat_routes * slots_per + slot_rank
    token_of = jnp.arange(flat_routes.shape[0], dtype=jnp.int32) // pairs
    outgoing = (
        jnp.zeros((experts * slots_per, normed.shape[1]), jnp.bfloat16)
        .at[slot_ids]
        .set(normed[token_of])
    )
    arrived = lax.all_to_all(outgoing, "sp", split_axis=0, concat_axis=0, tiled=True)
    inputs = lax.all_gather(arrived, "tp", axis=1, tiled=True)
    gate_part = jnp.dot(inputs, w_gate[0], preferred_element_type=jnp.float32)
    up_part = jnp.dot(inputs, w_up[0], preferred_element_type=jnp.float32)
    hidden = (jax.nn.silu(gate_part) * up_part).astype(jnp.bfloat16)
    down_part = w_down[0]
    result = jnp.dot(
        lax.all_gather(hidden, "tp", axis=1, tiled=True),
        down_part,
        preferred_element_type=jnp.float32,
    )
    returned = lax.all_to_all(
        result.astype(jnp.bfloat16), "sp", split_axis=0, concat_axis=0, tiled=True
    )
    picked = returned[slot_ids].astype(jnp.float32).reshape(positions, pairs, returned.shape[1])
    moe_sum = jnp.sum(picked * route_weight[:, :, None], axis=1)
    final_rows = ALPHA * normed.astype(jnp.float32) + moe_sum
    second_totals = lax.psum(
        (jnp.sum(final_rows, axis=1), jnp.sum(final_rows * final_rows, axis=1)), "tp"
    )
    return apply_norm(final_rows, second_totals, second_gain, second_bias, features).astype(
        jnp.bfloat16
    )


NT = (((1,), (1,)), ((), ()))
F32 = jnp.float32
BF16 = jnp.bfloat16
LANES = 128


def dot_nt(a, b):
    return lax.dot_general(a, b, NT, preferred_element_type=F32)


def dot_nn(a, b):
    return jnp.dot(a, b, preferred_element_type=F32)


def layout():
    sp, tp = lax.axis_index("sp"), lax.axis_index("tp")
    plane, core = sp // 2, lax.rem(sp, 2)
    y, x = tp // 2, lax.rem(tp, 2)
    return plane, core, y, x


def near_peers():
    tp = lax.axis_index("tp")
    beside = tp + 1 - 2 * lax.rem(tp, 2)
    return beside, lax.rem(tp + 2, 4), lax.rem(beside + 2, 4)


def enter(n_sp):
    sp = lax.axis_index("sp")
    beside, below, far = near_peers()
    barrier = pltpu.get_barrier_semaphore()
    for d in range(n_sp):
        if d:
            pl.semaphore_signal(barrier, inc=1, device_id={"sp": lax.rem(sp + d, n_sp)})
        pl.semaphore_signal(
            barrier, inc=1, device_id={"sp": lax.rem(sp + d, n_sp), "tp": beside}
        )
    for peer in (below, far):
        pl.semaphore_signal(barrier, inc=1, device_id={"tp": peer})
    pl.semaphore_wait(barrier, 2 * n_sp + 1)


def remote_to(src, dst, send, recv, device):
    return pltpu.make_async_remote_copy(
        src_ref=src, dst_ref=dst, send_sem=send, recv_sem=recv, device_id=device
    )


def remote(src, dst, send, recv, axis, peer):
    return remote_to(src, dst, send, recv, {axis: peer})


def share(buf, axis, n, send, recv):
    me = lax.axis_index(axis)
    for d in range(1, n):
        remote(
            buf.at[me], buf.at[me], send.at[d], recv.at[me], axis, lax.rem(me + d, n)
        ).start()


def collect(buf, axis, n, send, recv):
    me = lax.axis_index(axis)
    for d in range(1, n):
        other = lax.rem(me + d, n)
        remote(buf.at[other], buf.at[other], send.at[d], recv.at[other], axis, other).wait_recv()


def settle(buf, axis, n, send, recv):
    me = lax.axis_index(axis)
    for d in range(1, n):
        remote(
            buf.at[me], buf.at[me], send.at[d], recv.at[me], axis, lax.rem(me + d, n)
        ).wait_send()


def row_totals(rows, stats, n_tp, send, recv):
    me = lax.axis_index("tp")
    lane = lax.broadcasted_iota(jnp.int32, (rows.shape[0], LANES), 1)
    first = jnp.sum(rows, axis=1, keepdims=True)
    second = jnp.sum(rows * rows, axis=1, keepdims=True)
    both = jnp.where(lane == 0, first, jnp.where(lane == 1, second, 0.0))
    stats[me] = jnp.transpose(both)[:8]
    share(stats, "tp", n_tp, send, recv)
    collect(stats, "tp", n_tp, send, recv)
    total = stats[0]
    for k in range(1, n_tp):
        total = total + stats[k]
    total = jnp.concatenate([total, jnp.zeros((LANES - 8, total.shape[1]), F32)], axis=0)
    columns = jnp.transpose(total)
    return columns[:, 0:1], columns[:, 1:2]


def normalise(rows, totals, gain, bias, features):
    mean = totals[0] / features
    var = totals[1] / features - mean * mean
    return (rows - mean) * lax.rsqrt(var + EPS) * gain + bias


def layer_kernel(
    n_sp, n_tp, pool, doc_row, route_row, weight_row, pool_map, scale, gain, bias, gain2, bias2,
    w_out_hbm, gate_hbm, residual_hbm, w_gate_hbm, w_up_hbm, w_down_hbm, out,
    w_out, gate, residual, w_gate, w_up, w_down,
    halo, halo_ids, tails, mapped, stats, stats2, tables, blocks,
    aside, inputs, hidden, result, back, load_sem, w_send, w_recv,
    halo_send, halo_recv, tail_send, tail_recv, map_send, map_recv, stat_send, stat_recv,
    t_send, t_recv, z_send, z_recv, a_send, a_recv, y_send, y_recv, d_send, d_recv,
    h_send, h_recv, r_send, r_recv, stat2_send, stat2_recv,
):
    sp, tp = lax.axis_index("sp"), lax.axis_index("tp")
    plane, core, y, x = layout()
    partner = sp + 1 - 2 * core
    beside, below, far = near_peers()
    n_z = n_sp // 2
    steps = 2 * n_z
    channels, positions = pool.shape
    part = residual.shape[1]
    half = aside.shape[1]
    slots = 2 * half
    features = part * n_tp
    toward = 1 - 2 * (plane // (n_z // 2))
    straight = x == core
    expert = 2 * plane + x
    loads = [
        pltpu.make_async_copy(src, dst, load_sem.at[i])
        for i, (src, dst) in enumerate([
            (w_out_hbm, w_out), (gate_hbm, gate), (residual_hbm, residual),
        ])
    ]
    for load in loads:
        load.start()
    pieces = []
    for pair, cuts in ((((w_gate_hbm, w_gate), (w_up_hbm, w_up)), 4), (((w_down_hbm, w_down),), 4)):
        for cut in range(cuts):
            for src, dst in pair:
                size = dst.shape[0] // cuts
                span = pl.ds(cut * size, size)
                pieces.append((src.at[span], dst.at[span]))
    crossing = [
        remote_to(
            src, dst, w_send.at[i], w_recv.at[i],
            {"sp": 2 * plane + x, "tp": 2 * y + core},
        )
        for i, (src, dst) in enumerate(pieces)
    ]
    staying = [
        pltpu.make_async_copy(src, dst, w_recv.at[i]) for i, (src, dst) in enumerate(pieces)
    ]

    @pl.when(straight)
    def _():
        for copy in staying:
            copy.start()

    def cross(first, last):
        @pl.when(jnp.logical_not(straight))
        def _():
            for copy in crossing[first:last]:
                copy.start()

    def weights_here(first, last):
        @pl.when(straight)
        def _():
            for copy in staying[first:last]:
                copy.wait()

        @pl.when(jnp.logical_not(straight))
        def _():
            for copy in crossing[first:last]:
                copy.wait_recv()

    enter(n_sp)
    after = lax.rem(sp + 1, n_sp)
    last = pl.ds(positions - LANES, LANES)
    edge = remote(pool.at[:, last], halo, halo_send.at[0], halo_recv.at[0], "sp", after)
    edge_ids = remote(doc_row.at[:, last], halo_ids, halo_send.at[1], halo_recv.at[1], "sp", after)
    edge.start()
    edge_ids.start()
    cross(0, 3)
    ids = doc_row[...].astype(F32)
    in_last = (ids == ids[:, positions - 1 :]).astype(F32)
    tail = dot_nt(jnp.broadcast_to(in_last, (8, positions)).astype(BF16), pool[...])
    kind = lax.broadcasted_iota(jnp.int32, tail.shape, 0)
    tail = jnp.where(kind == 1, jnp.sum(in_last, axis=1, keepdims=True), tail)
    tails[sp] = jnp.where(kind == 2, ids[:, positions - 1 :], tail)
    share(tails, "sp", n_sp, tail_send, tail_recv)
    kind = lax.broadcasted_iota(jnp.int32, (LANES, positions), 0)
    later = lax.broadcasted_iota(jnp.int32, (positions, positions), 1)
    earlier = lax.broadcasted_iota(jnp.int32, (positions, positions), 0)
    ahead = (earlier < later).astype(F32).astype(BF16)
    r0, r1 = route_row[0:1], route_row[1:2]
    named = ((r0 == kind) | (r1 == kind)).astype(F32).astype(BF16)
    rank = dot_nn(named, ahead) + (kind * slots).astype(F32)
    slot0 = jnp.sum(jnp.where(r0 == kind, rank, 0.0), axis=0, keepdims=True)
    slot1 = jnp.sum(jnp.where(r1 == kind, rank, 0.0), axis=0, keepdims=True)
    table = jnp.where(kind == 0, slot0, jnp.where(kind == 1, slot1, 0.0))
    for i, row in enumerate((ids, weight_row[0:1], weight_row[1:2])):
        table = jnp.where(kind == i + 2, row, table)
    tables[plane] = table[:8]

    def table_copy(d):
        to = lax.rem(plane + d, n_z)
        return remote(
            tables.at[plane], tables.at[plane], t_send.at[d], t_recv.at[plane], "sp", 2 * to + core
        )

    for d in range(1, n_z):
        table_copy(d).start()
    columns = jnp.transpose(table)
    col = columns[:, 2:3]
    place = lax.broadcasted_iota(jnp.int32, (positions, LANES + positions), 1) - LANES
    delta = lax.broadcasted_iota(jnp.int32, (positions, LANES + positions), 0) - place
    edge.wait_recv()
    edge_ids.wait_recv()
    ext = jnp.concatenate([halo[...], pool[...]], axis=1)
    before = jnp.where(sp == 0, -1.0, halo_ids[...].astype(F32))
    ext_ids = jnp.concatenate([before, ids], axis=1)
    together = (col == ext_ids) & (delta >= 0)
    own = (delta == 0).astype(F32).astype(BF16)
    values = dot_nt(own, ext)
    sums, counts, wholes = [], [], []
    per = channels // GROUP_W
    for i in range(per):
        group = tp * per + i
        whole = lax.rem(group, 2) == 1
        window = jnp.left_shift(2, lax.rem(group // 2, 4))
        reach = jnp.where(whole, positions, window)
        least = jnp.where(whole, 0, -LANES)
        mask = (together & (delta < reach) & (place >= least)).astype(F32)
        sums.append(dot_nt(mask.astype(BF16), ext[i * GROUP_W : (i + 1) * GROUP_W]))
        counts.append(jnp.sum(mask, axis=1, keepdims=True))
        wholes.append(whole)
    collect(tails, "sp", n_sp, tail_send, tail_recv)
    opening = col[0:1]
    carry = jnp.zeros((1, channels), F32)
    carry_count = jnp.zeros((1, channels), F32)
    for k in range(n_sp - 1):
        block = tails[k]
        joins = (block[2:3] == opening) & (k < sp)
        carry = carry + jnp.where(joins, block[0:1], 0.0)
        carry_count = carry_count + jnp.where(joins, block[1:2], 0.0)
    goes_on = (col == opening).astype(F32)
    for i in range(per):
        group = tp * per + i
        span = slice(i * GROUP_W, (i + 1) * GROUP_W)
        joined = jnp.where(wholes[i], goes_on, 0.0)
        total = sums[i] + joined * carry[:, span]
        count = counts[i] + joined * carry_count[:, span]
        pooled = (total / count - values[:, span]).astype(BF16)
        factor = scale[:, pl.ds(pl.multiple_of(tp * channels, LANES), channels)][:, span]
        mapped[tp, :, span] = (dot_nn(pooled, pool_map[group]) * factor).astype(BF16)
    share(mapped, "tp", n_tp, map_send, map_recv)
    cross(3, 5)
    for load in loads:
        load.wait()
    opened = jax.nn.sigmoid(gate[...].astype(F32))
    kept = ALPHA * residual[...].astype(F32)
    collect(mapped, "tp", n_tp, map_send, map_recv)
    every = jnp.concatenate([mapped[k] for k in range(n_tp)], axis=1)
    rows = kept + dot_nn(every, w_out[...]) * opened
    totals = row_totals(rows, stats, n_tp, stat_send, stat_recv)
    blocks[plane] = normalise(rows, totals, gain[...], bias[...], features).astype(BF16)

    def unit_plane(m):
        return lax.rem(plane + toward * m + n_z, n_z)

    def hop(u, to, slot):
        return remote(
            blocks.at[u], blocks.at[u], z_send.at[slot], z_recv.at[u], "sp", 2 * to + core
        )

    def z_round(d):
        left, right = plane - d, plane + d

        @pl.when(left >= 0)
        def _():
            hop(left, plane, left).wait_recv()

            @pl.when(plane < n_z - 1)
            def _():
                hop(left, plane + 1, left).start()

        @pl.when(right < n_z)
        def _():
            hop(right, plane, right).wait_recv()

            @pl.when(plane > 0)
            def _():
                hop(right, plane - 1, right).start()

    def aside_copy(i):
        return remote(
            aside.at[i], inputs.at[i, core, tp], a_send.at[i], a_recv.at[i], "tp", beside
        )

    def down_y(i, k, which):
        ref = inputs.at[i, core, which]
        return remote(ref, ref, y_send.at[i, k], y_recv.at[i, k], "tp", below)

    def over(i, k, which, owner):
        ref = inputs.at[i, owner, which]
        return remote(ref, ref, d_send.at[i, k], d_recv.at[i, k], "sp", partner)

    def pack(m):
        u = unit_plane(m)
        slot_rows = tables[u]
        line = lax.broadcasted_iota(jnp.int32, (slots, positions), 0)

        def pick(e):
            mine = (line + e * slots).astype(F32)
            hit = (mine == slot_rows[0:1]) | (mine == slot_rows[1:2])
            return dot_nn(hit.astype(F32).astype(BF16), blocks[u]).astype(BF16)

        away = pick(2 * plane + 1 - x)
        for h in range(2):
            aside[2 * m + h] = away[h * half : (h + 1) * half]
            aside_copy(2 * m + h).start()
        kept_rows = pick(expert)
        for h in range(2):
            i = 2 * m + h
            inputs[i, core, tp] = kept_rows[h * half : (h + 1) * half]
            down_y(i, 0, tp).start()
            over(i, 0, tp, core).start()

    def beside_arrived(i):
        remote(
            aside.at[i], inputs.at[i, core, beside], a_send.at[i], a_recv.at[i], "tp", beside
        ).wait_recv()
        down_y(i, 1, beside).start()
        over(i, 1, beside, core).start()

    def below_arrived(i):
        for k, which in enumerate((below, far)):
            down_y(i, k, which).wait_recv()
            over(i, 2 + k, which, core).start()

    quarter = 2 * y + core

    def hidden_over(i, k, q):
        ref = hidden.at[i, q]
        return remote(ref, ref, h_send.at[i, k], h_recv.at[i, k], "sp", partner)

    def hidden_down(i, q):
        ref = hidden.at[i, q]
        return remote(ref, ref, h_send.at[i, 1], h_recv.at[i, 1], "tp", below)

    def expand(i):
        for k, which in enumerate((tp, beside, below, far)):
            over(i, k, which, 1 - core).wait_recv()
        rows = jnp.concatenate(
            [inputs[i, :, k].reshape(slots, part) for k in range(n_tp)], axis=1
        )
        gated = dot_nn(rows, w_gate[...])
        up = dot_nn(rows, w_up[...])
        hidden[i, quarter] = (gated * jax.nn.sigmoid(gated) * up).astype(BF16)
        hidden_down(i, quarter).start()
        hidden_over(i, 0, quarter).start()

    q_partner = 2 * y + 1 - core
    q_below = 2 * (1 - y) + core
    q_far = 2 * (1 - y) + 1 - core

    def is_own(i, c):
        return (i < 2) & straight & (core == c)

    def result_copy(i, c):
        u = unit_plane(i // 2)
        return remote_to(
            result.at[i, c], back.at[expert, lax.rem(i, 2)], r_send.at[i, c],
            r_recv.at[expert, lax.rem(i, 2)], {"sp": 2 * u + c, "tp": 2 * y + core},
        )

    def contract(i):
        hidden_down(i, q_below).wait_recv()
        hidden_over(i, 2, q_below).start()
        hidden_over(i, 0, q_partner).wait_recv()
        hidden_over(i, 2, q_far).wait_recv()
        rows = jnp.concatenate([hidden[i, k] for k in range(n_tp)], axis=1)
        block = dot_nn(rows, w_down[...]).astype(BF16)
        for c in range(2):
            result[i, c] = block[c * half : (c + 1) * half]

            @pl.when(jnp.logical_not(is_own(i, c)))
            def _():
                result_copy(i, c).start()

            @pl.when(is_own(i, c))
            def _():
                back[expert, lax.rem(i, 2)] = block[c * half : (c + 1) * half]

    @pl.when(plane < n_z - 1)
    def _():
        hop(plane, plane + 1, plane).start()

    @pl.when(plane > 0)
    def _():
        hop(plane, plane - 1, n_z).start()

    pack(0)
    cross(5, 8)
    for d in range(1, n_z):
        other = lax.rem(plane + d, n_z)
        remote(
            tables.at[other], tables.at[other], t_send.at[d], t_recv.at[other], "sp", partner
        ).wait_recv()
    beside_arrived(0)
    beside_arrived(1)
    z_round(1)
    pack(1)
    cross(8, 12)

    def step(n, _):
        s = lax.rem(n + 2, steps)
        first = lax.rem(n, 2) == 0

        @pl.when(first & (n < steps - 2))
        def _():
            beside_arrived(s)
            beside_arrived(s + 1)

        @pl.when(n == 0)
        def _():
            weights_here(0, 8)

        @pl.when(n < steps)
        def _():
            below_arrived(s)
            expand(s)

        @pl.when(first & (n < steps - 4))
        def _():
            z_round(n // 2 + 2)
            pack(n // 2 + 2)

        @pl.when(n == 1)
        def _():
            weights_here(8, 12)

        @pl.when(n > 0)
        def _():
            contract(lax.rem(n + 1, steps))

        return 0

    lax.fori_loop(0, steps + 1, step, 0)
    at0, at1 = columns[:, 0:1], columns[:, 1:2]
    spot = lax.broadcasted_iota(jnp.int32, (positions, 2 * slots), 1)
    sum0 = jnp.zeros((positions, part), F32)
    sum1 = jnp.zeros((positions, part), F32)
    for d in range(1, n_z + 1):
        u = lax.rem(plane + d, n_z)
        for side in range(2):
            e = 2 * u + side
            local = (u == plane) & straight & (x == side)

            @pl.when(jnp.logical_not(local))
            def _():
                for h in range(2):
                    remote(
                        result.at[0, 0], back.at[e, h], r_send.at[0, 0], r_recv.at[e, h],
                        "sp", partner,
                    ).wait_recv()

        returned = back[pl.ds(2 * u, 2)].reshape(2 * slots, part)
        spots = (spot + 2 * slots * u).astype(F32)
        sum0 = sum0 + dot_nn((spots == at0).astype(F32).astype(BF16), returned)
        sum1 = sum1 + dot_nn((spots == at1).astype(F32).astype(BF16), returned)
    moe = columns[:, 3:4] * sum0 + columns[:, 4:5] * sum1
    rows = ALPHA * blocks[plane].astype(F32) + moe
    totals = row_totals(rows, stats2, n_tp, stat2_send, stat2_recv)
    out[...] = normalise(rows, totals, gain2[...], bias2[...], features).astype(BF16)

    def drain(i, _):
        aside_copy(i).wait_send()
        for k, which in enumerate((tp, beside)):
            down_y(i, k, which).wait_send()
        for k, which in enumerate((tp, beside, below, far)):
            over(i, k, which, core).wait_send()
        hidden_down(i, quarter).wait_send()
        hidden_over(i, 0, quarter).wait_send()
        hidden_over(i, 2, q_below).wait_send()
        for c in range(2):
            @pl.when(jnp.logical_not(is_own(i, c)))
            def _():
                result_copy(i, c).wait_send()

        return 0

    lax.fori_loop(0, steps, drain, 0)

    @pl.when(jnp.logical_not(straight))
    def _():
        for copy in crossing:
            copy.wait_send()

    @pl.when(plane < n_z - 1)
    def _():
        hop(plane, plane + 1, plane).wait_send()
        for d in range(1, n_z - 1):
            @pl.when(plane - d >= 0)
            def _():
                hop(plane - d, plane + 1, plane - d).wait_send()

    @pl.when(plane > 0)
    def _():
        hop(plane, plane - 1, n_z).wait_send()
        for d in range(1, n_z - 1):
            @pl.when(plane + d < n_z)
            def _():
                hop(plane + d, plane - 1, plane + d).wait_send()

    for d in range(1, n_z):
        table_copy(d).wait_send()
    edge.wait_send()
    edge_ids.wait_send()
    settle(tails, "sp", n_sp, tail_send, tail_recv)
    settle(mapped, "tp", n_tp, map_send, map_recv)
    settle(stats, "tp", n_tp, stat_send, stat_recv)
    settle(stats2, "tp", n_tp, stat2_send, stat2_recv)


def body(n_sp, n_tp, *args):
    (pool_in, doc_ids, pool_map, pool_scale, w_out, gate_logit, residual, first_gain, first_bias,
     routes, route_weight, w_gate, w_up, w_down, second_gain, second_bias) = args
    channels, positions = pool_in.shape
    part = residual.shape[1]
    pairs = routes.shape[1]
    slots = 2 * positions * pairs // n_sp
    units = w_gate.shape[2]
    small = n_sp in (8, 12, 16) and n_sp % 4 == 0 and n_tp == 4 and pairs == 2 and slots % 32 == 0
    if not small or channels % LANES or positions % LANES or part % LANES or units % LANES:
        return general_body(*args)
    dma = pltpu.SemaphoreType.DMA
    n_z = n_sp // 2
    steps = 2 * n_z
    half = slots // 2
    loaded = (w_out, gate_logit, residual, w_gate[0], w_up[0], w_down[0])
    vmem = pl.BlockSpec(memory_space=pltpu.VMEM)
    any_space = pl.BlockSpec(memory_space=pl.ANY)
    return pl.pallas_call(
        functools.partial(layer_kernel, n_sp, n_tp),
        out_shape=jax.ShapeDtypeStruct(residual.shape, BF16),
        in_specs=[vmem] * 10 + [any_space] * len(loaded),
        out_specs=vmem,
        scratch_shapes=[
            *(pltpu.VMEM(x.shape, x.dtype) for x in loaded),
            pltpu.VMEM((channels, LANES), BF16),
            pltpu.VMEM((1, LANES), jnp.int32),
            pltpu.VMEM((n_sp, 8, channels), F32),
            pltpu.VMEM((n_tp, positions, channels), BF16),
            pltpu.VMEM((n_tp, 8, positions), F32),
            pltpu.VMEM((n_tp, 8, positions), F32),
            pltpu.VMEM((n_z, 8, positions), F32),
            pltpu.VMEM((n_z, positions, part), BF16),
            pltpu.VMEM((steps, half, part), BF16),
            pltpu.VMEM((steps, 2, n_tp, half, part), BF16),
            pltpu.VMEM((steps, n_tp, slots, units), BF16),
            pltpu.VMEM((steps, 2, half, part), BF16),
            pltpu.VMEM((n_sp, 2, half, part), BF16),
            dma((3,)), dma((12,)), dma((12,)),
            dma((2,)), dma((2,)), dma((n_sp,)), dma((n_sp,)),
            dma((n_tp,)), dma((n_tp,)), dma((n_tp,)), dma((n_tp,)),
            dma((n_z,)), dma((n_z,)), dma((n_z + 1,)), dma((n_z,)),
            dma((steps,)), dma((steps,)), dma((steps, 2)), dma((steps, 2)),
            dma((steps, 4)), dma((steps, 4)), dma((steps, 3)), dma((steps, 3)),
            dma((steps, 2)), dma((n_sp, 2)),
            dma((n_tp,)), dma((n_tp,)),
        ],
        compiler_params=pltpu.CompilerParams(
            collective_id=0, has_side_effects=True, vmem_limit_bytes=60 << 20
        ),
    )(
        pool_in, doc_ids[None], routes.T, route_weight.T, pool_map, pool_scale[None],
        first_gain[None], first_bias[None], second_gain[None], second_bias[None], *loaded,
    )


def solution(mesh):
    return jax.shard_map(
        functools.partial(body, mesh.shape["sp"], mesh.shape["tp"]),
        mesh=mesh,
        in_specs=(
            P("tp", "sp"),
            P("sp"),
            P(),
            P(),
            P(None, "tp"),
            P("sp", "tp"),
            P("sp", "tp"),
            P("tp"),
            P("tp"),
            P("sp", None),
            P("sp", None),
            P("sp", None, "tp"),
            P("sp", None, "tp"),
            P("sp", None, "tp"),
            P("tp"),
            P("tp"),
        ),
        out_specs=P("sp", "tp"),
        check_vma=False,
    )
```

```python
import functools

import jax
import jax.numpy as jnp
from jax import lax
from jax.experimental import pallas as pl
from jax.experimental.pallas import tpu as pltpu
from jax.sharding import PartitionSpec as P

GROUP_W = 64


EPS = 1e-05
ALPHA = 8.0**0.25
halo_len = 16


def shifted(shard, axis, by):
    size = lax.axis_size(axis)
    pairs = [(i, i + by) for i in range(size) if 0 <= i + by < size]
    return lax.ppermute(shard, axis, pairs)


def entering(shard, axis, combine, identity):
    size, place = (lax.axis_size(axis), lax.axis_index(axis))
    everything = jax.tree.map(lambda part: lax.all_gather(part, axis), shard)
    start = jax.tree.map(
        lambda part, zero: jnp.broadcast_to(jnp.asarray(zero, part.dtype), part.shape),
        shard,
        identity,
    )

    def turn(k, before):
        reached = k < place
        new = combine(before, jax.tree.map(lambda part: part[k], everything))
        return jax.tree.map(lambda a, b: jnp.where(reached, a, b), new, before)

    return lax.fori_loop(0, size, turn, start)


def carry_join(earlier, later):
    keeping = 1.0 - later[2]
    return (
        later[0] + keeping * earlier[0],
        later[1] + keeping * earlier[1],
        jnp.maximum(earlier[2], later[2]),
    )


def apply_norm(row_data, totals, gain_vec, bias_vec, features):
    row_mean = totals[0][:, None] / features
    row_var = totals[1][:, None] / features - row_mean * row_mean
    return (row_data - row_mean) * lax.rsqrt(row_var + EPS) * gain_vec + bias_vec


def pool_scales(pool_in, doc_ids):
    channels_dev, positions = pool_in.shape
    edge_block = jnp.concatenate(
        [
            pool_in[:, positions - halo_len :],
            doc_ids[None, positions - halo_len :].astype(jnp.bfloat16),
        ],
        axis=0,
    )
    previous = shifted(edge_block, "sp", 1)
    prior_ids = jnp.where(
        lax.axis_index("sp") == 0, -1.0, previous[channels_dev].astype(jnp.float32)
    )
    ids_ext = jnp.concatenate([prior_ids, doc_ids.astype(jnp.float32)])
    inputs_ext = jnp.concatenate([previous[:channels_dev], pool_in], axis=1).astype(jnp.float32)
    length = positions + halo_len
    opening = jnp.concatenate([jnp.zeros((1,), bool), ids_ext[1:] != ids_ext[:-1]])
    places = jnp.arange(length, dtype=jnp.int32)
    doc_start = lax.cummax(jnp.where(opening, places, 0), axis=0)
    prefix = jnp.concatenate(
        [jnp.zeros((channels_dev, 1), jnp.float32), jnp.cumsum(inputs_ext, axis=1)], axis=1
    )
    start_here = doc_start[halo_len:]
    upper_at = places[halo_len:] + 1
    at_start = jnp.take(prefix, start_here, axis=1)
    current = prefix[:, halo_len + 1 :]
    group_id = (
        lax.axis_index("tp") * channels_dev + jnp.arange(channels_dev, dtype=jnp.int32)
    ) // GROUP_W
    doc_mask = (group_id % 2 == 1)[:, None]
    window = jnp.left_shift(2, group_id // 2 % 4)[:, None]
    lagged = jnp.zeros((channels_dev, positions), jnp.float32)
    for octave in range(4):
        window_len = 2 << octave
        begin = halo_len + 1 - window_len
        lagged = lagged + jnp.where(window == window_len, prefix[:, begin : begin + positions], 0.0)
    lower_at = jnp.maximum(upper_at[None, :] - window, start_here[None, :])
    win_sum = current - jnp.where(
        start_here[None, :] > upper_at[None, :] - window, at_start, lagged
    )
    win_count = (upper_at[None, :] - lower_at).astype(jnp.float32)
    opened = start_here >= halo_len
    local_sum = current - jnp.where(opened[None, :], at_start, prefix[:, halo_len : halo_len + 1])
    local_count = (upper_at - jnp.maximum(start_here, halo_len)).astype(jnp.float32)
    last_start = doc_start[length - 1]
    last_base = jnp.where(
        last_start >= halo_len,
        lax.dynamic_slice_in_dim(prefix, last_start, 1, 1)[:, 0],
        prefix[:, halo_len],
    )
    summary = (
        prefix[:, length] - last_base,
        (length - jnp.maximum(last_start, halo_len)).astype(jnp.float32),
        (last_start >= halo_len).astype(jnp.float32),
    )
    nothing = (jnp.zeros((channels_dev,), jnp.float32), jnp.float32(0.0), jnp.float32(0.0))
    carried = entering(summary, "sp", carry_join, nothing)
    doc_sum = local_sum + jnp.where(opened[None, :], 0.0, carried[0][:, None])
    doc_count = local_count + jnp.where(opened, 0.0, carried[1])
    pooled = (
        jnp.where(doc_mask, doc_sum / doc_count[None, :], win_sum / win_count)
        - inputs_ext[:, halo_len:]
    )
    return pooled.astype(jnp.bfloat16)


def general_body(
    pool_in,
    doc_ids,
    pool_map,
    pool_scale,
    w_out,
    gate_logit,
    residual,
    first_gain,
    first_bias,
    routes,
    route_weight,
    w_gate,
    w_up,
    w_down,
    second_gain,
    second_bias,
):
    pooled = pool_scales(pool_in, doc_ids)
    positions = pool_in.shape[1]
    features = residual.shape[1] * lax.axis_size("tp")
    gathered = lax.all_gather(pooled, "tp", axis=0, tiled=True)
    group_count = gathered.shape[0] // GROUP_W
    grouped = jnp.einsum(
        "gct,gcd->tgd",
        gathered.reshape(group_count, GROUP_W, positions),
        pool_map,
        preferred_element_type=jnp.float32,
    )
    mapped = (grouped.reshape(positions, group_count * GROUP_W) * pool_scale).astype(jnp.bfloat16)
    mixer_out = jnp.dot(mapped, w_out, preferred_element_type=jnp.float32) * jax.nn.sigmoid(
        gate_logit.astype(jnp.float32)
    )
    mixed_rows = ALPHA * residual.astype(jnp.float32) + mixer_out
    first_totals = lax.psum(
        (jnp.sum(mixed_rows, axis=1), jnp.sum(mixed_rows * mixed_rows, axis=1)), "tp"
    )
    normed = apply_norm(mixed_rows, first_totals, first_gain, first_bias, features).astype(
        jnp.bfloat16
    )
    experts = lax.axis_size("sp")
    pairs = routes.shape[1]
    slots_per = 2 * positions * pairs // experts
    flat_routes = routes.reshape(-1)
    one_hot = (flat_routes[:, None] == jnp.arange(experts, dtype=jnp.int32)[None, :]).astype(
        jnp.int32
    )
    slot_rank = jnp.sum((jnp.cumsum(one_hot, axis=0, dtype=jnp.int32) - 1) * one_hot, axis=1)
    slot_ids = flat_routes * slots_per + slot_rank
    token_of = jnp.arange(flat_routes.shape[0], dtype=jnp.int32) // pairs
    outgoing = (
        jnp.zeros((experts * slots_per, normed.shape[1]), jnp.bfloat16)
        .at[slot_ids]
        .set(normed[token_of])
    )
    arrived = lax.all_to_all(outgoing, "sp", split_axis=0, concat_axis=0, tiled=True)
    inputs = lax.all_gather(arrived, "tp", axis=1, tiled=True)
    gate_part = jnp.dot(inputs, w_gate[0], preferred_element_type=jnp.float32)
    up_part = jnp.dot(inputs, w_up[0], preferred_element_type=jnp.float32)
    hidden = (jax.nn.silu(gate_part) * up_part).astype(jnp.bfloat16)
    down_part = w_down[0]
    result = jnp.dot(
        lax.all_gather(hidden, "tp", axis=1, tiled=True),
        down_part,
        preferred_element_type=jnp.float32,
    )
    returned = lax.all_to_all(
        result.astype(jnp.bfloat16), "sp", split_axis=0, concat_axis=0, tiled=True
    )
    picked = returned[slot_ids].astype(jnp.float32).reshape(positions, pairs, returned.shape[1])
    moe_sum = jnp.sum(picked * route_weight[:, :, None], axis=1)
    final_rows = ALPHA * normed.astype(jnp.float32) + moe_sum
    second_totals = lax.psum(
        (jnp.sum(final_rows, axis=1), jnp.sum(final_rows * final_rows, axis=1)), "tp"
    )
    return apply_norm(final_rows, second_totals, second_gain, second_bias, features).astype(
        jnp.bfloat16
    )


NT = (((1,), (1,)), ((), ()))
F32 = jnp.float32
BF16 = jnp.bfloat16
LANES = 128


def dot_nt(a, b):
    return lax.dot_general(a, b, NT, preferred_element_type=F32)


def dot_nn(a, b):
    return jnp.dot(a, b, preferred_element_type=F32)


def layout():
    sp, tp = lax.axis_index("sp"), lax.axis_index("tp")
    plane, core = sp // 2, lax.rem(sp, 2)
    y, x = tp // 2, lax.rem(tp, 2)
    return plane, core, y, x


def near_peers():
    tp = lax.axis_index("tp")
    beside = tp + 1 - 2 * lax.rem(tp, 2)
    return beside, lax.rem(tp + 2, 4), lax.rem(beside + 2, 4)


def greet(n_sp):
    sp = lax.axis_index("sp")
    beside, below, far = near_peers()
    barrier = pltpu.get_barrier_semaphore()
    for d in range(n_sp):
        if d:
            pl.semaphore_signal(barrier, inc=1, device_id={"sp": lax.rem(sp + d, n_sp)})
        pl.semaphore_signal(
            barrier, inc=1, device_id={"sp": lax.rem(sp + d, n_sp), "tp": beside}
        )
    for peer in (below, far):
        pl.semaphore_signal(barrier, inc=1, device_id={"tp": peer})


def all_here(n_sp):
    pl.semaphore_wait(pltpu.get_barrier_semaphore(), 2 * n_sp + 1)


def remote_to(src, dst, send, recv, device):
    return pltpu.make_async_remote_copy(
        src_ref=src, dst_ref=dst, send_sem=send, recv_sem=recv, device_id=device
    )


def remote(src, dst, send, recv, axis, peer):
    return remote_to(src, dst, send, recv, {axis: peer})


def share(buf, axis, n, send, recv):
    me = lax.axis_index(axis)
    for d in range(1, n):
        remote(
            buf.at[me], buf.at[me], send.at[d], recv.at[me], axis, lax.rem(me + d, n)
        ).start()


def collect(buf, axis, n, send, recv):
    me = lax.axis_index(axis)
    for d in range(1, n):
        other = lax.rem(me + d, n)
        remote(buf.at[other], buf.at[other], send.at[d], recv.at[other], axis, other).wait_recv()


def settle(buf, axis, n, send, recv):
    me = lax.axis_index(axis)
    for d in range(1, n):
        remote(
            buf.at[me], buf.at[me], send.at[d], recv.at[me], axis, lax.rem(me + d, n)
        ).wait_send()


def row_totals(rows, stats, n_tp, send, recv, between=None):
    me = lax.axis_index("tp")
    lane = lax.broadcasted_iota(jnp.int32, (rows.shape[0], LANES), 1)
    first = jnp.sum(rows, axis=1, keepdims=True)
    second = jnp.sum(rows * rows, axis=1, keepdims=True)
    both = jnp.where(lane == 0, first, jnp.where(lane == 1, second, 0.0))
    stats[me] = jnp.transpose(both)[:8]
    share(stats, "tp", n_tp, send, recv)
    if between is not None:
        between()
    collect(stats, "tp", n_tp, send, recv)
    total = stats[0]
    for k in range(1, n_tp):
        total = total + stats[k]
    total = jnp.concatenate([total, jnp.zeros((LANES - 8, total.shape[1]), F32)], axis=0)
    columns = jnp.transpose(total)
    return columns[:, 0:1], columns[:, 1:2]


def normalise(rows, totals, gain, bias, features):
    mean = totals[0] / features
    var = totals[1] / features - mean * mean
    return (rows - mean) * lax.rsqrt(var + EPS) * gain + bias


def layer_kernel(
    n_sp, n_tp, pool, doc_ids, route_row, weight_row, pool_map, scale, gain, bias, gain2, bias2,
    w_out_hbm, gate_hbm, residual_hbm, w_gate_hbm, w_up_hbm, w_down_hbm, out,
    w_out, gate, residual, w_gate, w_up, w_down,
    doc_row, halo, halo_ids, tails, mapped, stats, stats2, tables, blocks,
    aside, inputs, hidden, result, back, load_sem, w_send, w_recv,
    halo_send, halo_recv, tail_send, tail_recv, map_send, map_recv, stat_send, stat_recv,
    t_send, t_recv, z_send, z_recv, a_send, a_recv, y_send, y_recv, d_send, d_recv,
    h_send, h_recv, r_send, r_recv, stat2_send, stat2_recv,
):
    sp, tp = lax.axis_index("sp"), lax.axis_index("tp")
    plane, core, y, x = layout()
    partner = sp + 1 - 2 * core
    beside, below, far = near_peers()
    n_z = n_sp // 2
    steps = 2 * n_z
    channels, positions = pool.shape
    part = residual.shape[1]
    half = aside.shape[1]
    slots = 2 * half
    features = part * n_tp
    toward = 1 - 2 * (plane // (n_z // 2))
    straight = x == core
    shift = jnp.where((plane > 0) & (plane < n_z - 1), 1, 0)
    expert = 2 * plane + x
    loads = [
        pltpu.make_async_copy(src, dst, load_sem.at[i])
        for i, (src, dst) in enumerate([
            (w_out_hbm, w_out), (gate_hbm, gate), (residual_hbm, residual),
        ])
    ]
    for load in loads:
        load.start()
    pieces = []
    for pair, cuts in ((((w_gate_hbm, w_gate), (w_up_hbm, w_up)), 8), (((w_down_hbm, w_down),), 8)):
        for cut in range(cuts):
            for src, dst in pair:
                size = dst.shape[0] // cuts
                span = pl.ds(cut * size, size)
                pieces.append((src.at[span], dst.at[span]))
    crossing = [
        remote_to(
            src, dst, w_send.at[i], w_recv.at[i],
            {"sp": 2 * plane + x, "tp": 2 * y + core},
        )
        for i, (src, dst) in enumerate(pieces)
    ]
    staying = [
        pltpu.make_async_copy(src, dst, w_recv.at[i]) for i, (src, dst) in enumerate(pieces)
    ]

    @pl.when(straight)
    def _():
        for copy in staying:
            copy.start()

    def cross(first, last):
        @pl.when(jnp.logical_not(straight))
        def _():
            for copy in crossing[first:last]:
                copy.start()

    def weights_here(first, last):
        @pl.when(straight)
        def _():
            for copy in staying[first:last]:
                copy.wait()

        @pl.when(jnp.logical_not(straight))
        def _():
            for copy in crossing[first:last]:
                copy.wait_recv()

    greet(n_sp)
    doc_row[...] = doc_ids[...].reshape(1, positions)
    ids = doc_row[...].astype(F32)
    in_last = (ids == ids[:, positions - 1 :]).astype(F32)
    tail = dot_nt(jnp.broadcast_to(in_last, (8, positions)).astype(BF16), pool[...])
    kind = lax.broadcasted_iota(jnp.int32, tail.shape, 0)
    tail = jnp.where(kind == 1, jnp.sum(in_last, axis=1, keepdims=True), tail)
    tails[sp] = jnp.where(kind == 2, ids[:, positions - 1 :], tail)
    kind = lax.broadcasted_iota(jnp.int32, (LANES, positions), 0)
    later = lax.broadcasted_iota(jnp.int32, (positions, positions), 1)
    earlier = lax.broadcasted_iota(jnp.int32, (positions, positions), 0)
    ahead = (earlier < later).astype(F32).astype(BF16)
    r0, r1 = route_row[0:1], route_row[1:2]
    named = ((r0 == kind) | (r1 == kind)).astype(F32).astype(BF16)
    rank = dot_nn(named, ahead) + (kind * slots).astype(F32)
    slot0 = jnp.sum(jnp.where(r0 == kind, rank, 0.0), axis=0, keepdims=True)
    slot1 = jnp.sum(jnp.where(r1 == kind, rank, 0.0), axis=0, keepdims=True)
    table = jnp.where(kind == 0, slot0, jnp.where(kind == 1, slot1, 0.0))
    for i, row in enumerate((ids, weight_row[0:1], weight_row[1:2])):
        table = jnp.where(kind == i + 2, row, table)
    tables[plane] = table[:8]

    def table_copy(d):
        to = lax.rem(plane + d, n_z)
        return remote(
            tables.at[plane], tables.at[plane], t_send.at[d], t_recv.at[plane], "sp", 2 * to + core
        )

    columns = jnp.transpose(table)
    col = columns[:, 2:3]
    place = lax.broadcasted_iota(jnp.int32, (positions, LANES + positions), 1) - LANES
    delta = lax.broadcasted_iota(jnp.int32, (positions, LANES + positions), 0) - place
    all_here(n_sp)
    after = lax.rem(sp + 1, n_sp)
    last = pl.ds(positions - LANES, LANES)
    edge = remote(pool.at[:, last], halo, halo_send.at[0], halo_recv.at[0], "sp", after)
    edge_ids = remote(doc_row.at[:, last], halo_ids, halo_send.at[1], halo_recv.at[1], "sp", after)
    edge.start()
    edge_ids.start()
    share(tails, "sp", n_sp, tail_send, tail_recv)
    cross(0, 5)
    for d in range(1, n_z):
        table_copy(d).start()
    edge.wait_recv()
    edge_ids.wait_recv()
    ext = jnp.concatenate([halo[...], pool[...]], axis=1)
    before = jnp.where(sp == 0, -1.0, halo_ids[...].astype(F32))
    ext_ids = jnp.concatenate([before, ids], axis=1)
    together = (col == ext_ids) & (delta >= 0)
    own = (delta == 0).astype(F32).astype(BF16)
    values = dot_nt(own, ext)
    sums, counts, wholes = [], [], []
    per = channels // GROUP_W
    for i in range(per):
        group = tp * per + i
        whole = lax.rem(group, 2) == 1
        window = jnp.left_shift(2, lax.rem(group // 2, 4))
        reach = jnp.where(whole, positions, window)
        least = jnp.where(whole, 0, -LANES)
        mask = (together & (delta < reach) & (place >= least)).astype(F32)
        sums.append(dot_nt(mask.astype(BF16), ext[i * GROUP_W : (i + 1) * GROUP_W]))
        counts.append(jnp.sum(mask, axis=1, keepdims=True))
        wholes.append(whole)
    collect(tails, "sp", n_sp, tail_send, tail_recv)
    opening = col[0:1]
    carry = jnp.zeros((1, channels), F32)
    carry_count = jnp.zeros((1, channels), F32)
    for k in range(n_sp - 1):
        block = tails[k]
        joins = (block[2:3] == opening) & (k < sp)
        carry = carry + jnp.where(joins, block[0:1], 0.0)
        carry_count = carry_count + jnp.where(joins, block[1:2], 0.0)
    goes_on = (col == opening).astype(F32)
    for i in range(per):
        group = tp * per + i
        span = slice(i * GROUP_W, (i + 1) * GROUP_W)
        joined = jnp.where(wholes[i], goes_on, 0.0)
        total = sums[i] + joined * carry[:, span]
        count = counts[i] + joined * carry_count[:, span]
        pooled = (total / count - values[:, span]).astype(BF16)
        factor = scale[:, pl.ds(pl.multiple_of(tp * channels, LANES), channels)][:, span]
        mapped[tp, :, span] = (dot_nn(pooled, pool_map[group]) * factor).astype(BF16)
    share(mapped, "tp", n_tp, map_send, map_recv)
    cross(5, 7)
    for load in loads:
        load.wait()
    opened = jax.nn.sigmoid(gate[...].astype(F32))
    kept = ALPHA * residual[...].astype(F32)
    collect(mapped, "tp", n_tp, map_send, map_recv)
    every = jnp.concatenate([mapped[k] for k in range(n_tp)], axis=1)
    rows = kept + dot_nn(every, w_out[...]) * opened
    totals = row_totals(rows, stats, n_tp, stat_send, stat_recv, lambda: cross(7, 11))
    blocks[plane] = normalise(rows, totals, gain[...], bias[...], features).astype(BF16)

    def unit_plane(m):
        return lax.rem(plane + toward * (m + shift) + 2 * n_z, n_z)

    def packed_unit(p):
        return lax.rem(p - shift + n_z, n_z)

    def hop(u, to, slot):
        return remote(
            blocks.at[u], blocks.at[u], z_send.at[slot], z_recv.at[u], "sp", 2 * to + core
        )

    def z_round(d):
        left, right = plane - d, plane + d

        @pl.when(left >= 0)
        def _():
            hop(left, plane, left).wait_recv()

            @pl.when(plane < n_z - 1)
            def _():
                hop(left, plane + 1, left).start()

        @pl.when(right < n_z)
        def _():
            hop(right, plane, right).wait_recv()

            @pl.when(plane > 0)
            def _():
                hop(right, plane - 1, right).start()

    def aside_copy(i):
        return remote(
            aside.at[i], inputs.at[i, core, tp], a_send.at[i], a_recv.at[i], "tp", beside
        )

    def down_y(i, k, which):
        ref = inputs.at[i, core, which]
        return remote(ref, ref, y_send.at[i, k], y_recv.at[i, k], "tp", below)

    def over(i, k, which, owner):
        ref = inputs.at[i, owner, which]
        return remote(ref, ref, d_send.at[i, k], d_recv.at[i, k], "sp", partner)

    def pack(m):
        u = unit_plane(m)
        slot_rows = tables[u]
        line = lax.broadcasted_iota(jnp.int32, (slots, positions), 0)

        def pick(e):
            mine = (line + e * slots).astype(F32)
            hit = (mine == slot_rows[0:1]) | (mine == slot_rows[1:2])
            return dot_nn(hit.astype(F32).astype(BF16), blocks[u]).astype(BF16)

        away = pick(2 * plane + 1 - x)
        for h in range(2):
            aside[2 * m + h] = away[h * half : (h + 1) * half]
            aside_copy(2 * m + h).start()
        kept_rows = pick(expert)
        for h in range(2):
            i = 2 * m + h
            inputs[i, core, tp] = kept_rows[h * half : (h + 1) * half]
            down_y(i, 0, tp).start()
            over(i, 0, tp, core).start()

    def beside_arrived(i):
        remote(
            aside.at[i], inputs.at[i, core, beside], a_send.at[i], a_recv.at[i], "tp", beside
        ).wait_recv()
        down_y(i, 1, beside).start()
        over(i, 1, beside, core).start()

    def below_arrived(i):
        for k, which in enumerate((below, far)):
            down_y(i, k, which).wait_recv()
            over(i, 2 + k, which, core).start()

    quarter = 2 * y + core

    def hidden_over(i, k, q):
        ref = hidden.at[i, q]
        return remote(ref, ref, h_send.at[i, k], h_recv.at[i, k], "sp", partner)

    def hidden_down(i, q):
        ref = hidden.at[i, q]
        return remote(ref, ref, h_send.at[i, 1], h_recv.at[i, 1], "tp", below)

    def expand(i):
        for k, which in enumerate((tp, beside, below, far)):
            over(i, k, which, 1 - core).wait_recv()
        rows = jnp.concatenate(
            [inputs[i, :, k].reshape(slots, part) for k in range(n_tp)], axis=1
        )
        gated = dot_nn(rows, w_gate[...])
        up = dot_nn(rows, w_up[...])
        hidden[i, quarter] = (gated * jax.nn.sigmoid(gated) * up).astype(BF16)
        hidden_down(i, quarter).start()
        hidden_over(i, 0, quarter).start()

    q_partner = 2 * y + 1 - core
    q_below = 2 * (1 - y) + core
    q_far = 2 * (1 - y) + 1 - core

    def is_own(i, c):
        return (unit_plane(i // 2) == plane) & straight & (core == c)

    def result_copy(i, c):
        u = unit_plane(i // 2)
        return remote_to(
            result.at[i, c], back.at[expert, lax.rem(i, 2)], r_send.at[i, c],
            r_recv.at[expert, lax.rem(i, 2)], {"sp": 2 * u + c, "tp": 2 * y + core},
        )

    def below_hidden(i):
        hidden_down(i, q_below).wait_recv()
        hidden_over(i, 2, q_below).start()

    def contract(i):
        hidden_over(i, 0, q_partner).wait_recv()
        hidden_over(i, 2, q_far).wait_recv()
        rows = jnp.concatenate([hidden[i, k] for k in range(n_tp)], axis=1)
        block = dot_nn(rows, w_down[...]).astype(BF16)
        for c in range(2):
            result[i, c] = block[c * half : (c + 1) * half]

            @pl.when(jnp.logical_not(is_own(i, c)))
            def _():
                result_copy(i, c).start()

            @pl.when(is_own(i, c))
            def _():
                back[expert, lax.rem(i, 2)] = block[c * half : (c + 1) * half]

    @pl.when(plane < n_z - 1)
    def _():
        hop(plane, plane + 1, plane).start()

    @pl.when(plane > 0)
    def _():
        hop(plane, plane - 1, n_z).start()

    pack(packed_unit(0))
    cross(11, 16)
    for d in range(1, n_z):
        other = lax.rem(plane + d, n_z)
        remote(
            tables.at[other], tables.at[other], t_send.at[d], t_recv.at[other], "sp", partner
        ).wait_recv()

    def both_beside(p):
        i = 2 * packed_unit(p)
        beside_arrived(i)
        beside_arrived(i + 1)

    both_beside(0)
    z_round(1)
    pack(packed_unit(1))
    cross(16, 20)

    def step(p, _):
        @pl.when(p + 1 < n_z)
        def _():
            both_beside(p + 1)

        @pl.when(p + 2 < n_z)
        def _():
            z_round(p + 2)
            pack(packed_unit(p + 2))

        @pl.when(p == 0)
        def _():
            cross(20, 24)

        @pl.when(p == 1)
        def _():
            cross(24, 24)

        @pl.when(p > 0)
        def _():
            below_hidden(2 * p - 2)

        @pl.when(p > 0)
        def _():
            below_hidden(2 * p - 1)

        @pl.when(p == 1)
        def _():
            weights_here(16, 24)

        @pl.when(p > 0)
        def _():
            contract(2 * p - 2)

        @pl.when(p > 0)
        def _():
            contract(2 * p - 1)

        @pl.when(p == 0)
        def _():
            weights_here(0, 16)

        @pl.when(p < n_z)
        def _():
            below_arrived(2 * p + 0)
            expand(2 * p + 0)

        @pl.when(p < n_z)
        def _():
            below_arrived(2 * p + 1)
            expand(2 * p + 1)

        return 0

    lax.fori_loop(0, n_z + 1, step, 0)
    at0, at1 = columns[:, 0:1], columns[:, 1:2]
    spot = lax.broadcasted_iota(jnp.int32, (positions, 2 * slots), 1)
    sum0 = jnp.zeros((positions, part), F32)
    sum1 = jnp.zeros((positions, part), F32)
    inner = jnp.where((plane > 0) & (plane < n_z - 1), 1, 0)
    for d in range(n_z):
        u = lax.rem(plane + toward * (d + inner) + 2 * n_z, n_z)
        for side in range(2):
            e = 2 * u + side
            local = (u == plane) & straight & (x == side)

            @pl.when(jnp.logical_not(local))
            def _():
                for h in range(2):
                    remote(
                        result.at[0, 0], back.at[e, h], r_send.at[0, 0], r_recv.at[e, h],
                        "sp", partner,
                    ).wait_recv()

        returned = back[pl.ds(2 * u, 2)].reshape(2 * slots, part)
        spots = (spot + 2 * slots * u).astype(F32)
        sum0 = sum0 + dot_nn((spots == at0).astype(F32).astype(BF16), returned)
        sum1 = sum1 + dot_nn((spots == at1).astype(F32).astype(BF16), returned)
    moe = columns[:, 3:4] * sum0 + columns[:, 4:5] * sum1
    rows = ALPHA * blocks[plane].astype(F32) + moe
    totals = row_totals(rows, stats2, n_tp, stat2_send, stat2_recv)
    out[...] = normalise(rows, totals, gain2[...], bias2[...], features).astype(BF16)

    def drain(i, _):
        aside_copy(i).wait_send()
        for k, which in enumerate((tp, beside)):
            down_y(i, k, which).wait_send()
        for k, which in enumerate((tp, beside, below, far)):
            over(i, k, which, core).wait_send()
        hidden_down(i, quarter).wait_send()
        hidden_over(i, 0, quarter).wait_send()
        hidden_over(i, 2, q_below).wait_send()
        for c in range(2):
            @pl.when(jnp.logical_not(is_own(i, c)))
            def _():
                result_copy(i, c).wait_send()

        return 0

    lax.fori_loop(0, steps, drain, 0)

    @pl.when(jnp.logical_not(straight))
    def _():
        for copy in crossing:
            copy.wait_send()

    @pl.when(plane < n_z - 1)
    def _():
        hop(plane, plane + 1, plane).wait_send()
        for d in range(1, n_z - 1):
            @pl.when(plane - d >= 0)
            def _():
                hop(plane - d, plane + 1, plane - d).wait_send()

    @pl.when(plane > 0)
    def _():
        hop(plane, plane - 1, n_z).wait_send()
        for d in range(1, n_z - 1):
            @pl.when(plane + d < n_z)
            def _():
                hop(plane + d, plane - 1, plane + d).wait_send()

    for d in range(1, n_z):
        table_copy(d).wait_send()
    edge.wait_send()
    edge_ids.wait_send()
    settle(tails, "sp", n_sp, tail_send, tail_recv)
    settle(mapped, "tp", n_tp, map_send, map_recv)
    settle(stats, "tp", n_tp, stat_send, stat_recv)
    settle(stats2, "tp", n_tp, stat2_send, stat2_recv)


def body(n_sp, n_tp, *args):
    (pool_in, doc_ids, pool_map, pool_scale, w_out, gate_logit, residual, first_gain, first_bias,
     routes, route_weight, w_gate, w_up, w_down, second_gain, second_bias) = args
    channels, positions = pool_in.shape
    part = residual.shape[1]
    pairs = routes.shape[1]
    slots = 2 * positions * pairs // n_sp
    units = w_gate.shape[2]
    small = n_sp == 8 and n_tp == 4 and pairs == 2 and slots % 32 == 0
    if not small or channels % LANES or positions % LANES or part % LANES or units % LANES:
        return general_body(*args)
    dma = pltpu.SemaphoreType.DMA
    n_z = n_sp // 2
    steps = 2 * n_z
    half = slots // 2
    loaded = (w_out, gate_logit, residual, w_gate[0], w_up[0], w_down[0])
    vmem = pl.BlockSpec(memory_space=pltpu.VMEM)
    any_space = pl.BlockSpec(memory_space=pl.ANY)
    return pl.pallas_call(
        functools.partial(layer_kernel, n_sp, n_tp),
        out_shape=jax.ShapeDtypeStruct(residual.shape, BF16),
        in_specs=[vmem] * 10 + [any_space] * len(loaded),
        out_specs=vmem,
        scratch_shapes=[
            *(pltpu.VMEM(x.shape, x.dtype) for x in loaded),
            pltpu.VMEM((1, positions), jnp.int32),
            pltpu.VMEM((channels, LANES), BF16),
            pltpu.VMEM((1, LANES), jnp.int32),
            pltpu.VMEM((n_sp, 8, channels), F32),
            pltpu.VMEM((n_tp, positions, channels), BF16),
            pltpu.VMEM((n_tp, 8, positions), F32),
            pltpu.VMEM((n_tp, 8, positions), F32),
            pltpu.VMEM((n_z, 8, positions), F32),
            pltpu.VMEM((n_z, positions, part), BF16),
            pltpu.VMEM((steps, half, part), BF16),
            pltpu.VMEM((steps, 2, n_tp, half, part), BF16),
            pltpu.VMEM((steps, n_tp, slots, units), BF16),
            pltpu.VMEM((steps, 2, half, part), BF16),
            pltpu.VMEM((n_sp, 2, half, part), BF16),
            dma((3,)), dma((24,)), dma((24,)),
            dma((2,)), dma((2,)), dma((n_sp,)), dma((n_sp,)),
            dma((n_tp,)), dma((n_tp,)), dma((n_tp,)), dma((n_tp,)),
            dma((n_z,)), dma((n_z,)), dma((n_z + 1,)), dma((n_z,)),
            dma((steps,)), dma((steps,)), dma((steps, 2)), dma((steps, 2)),
            dma((steps, 4)), dma((steps, 4)), dma((steps, 3)), dma((steps, 3)),
            dma((steps, 2)), dma((n_sp, 2)),
            dma((n_tp,)), dma((n_tp,)),
        ],
        compiler_params=pltpu.CompilerParams(
            collective_id=0, has_side_effects=True, vmem_limit_bytes=60 << 20
        ),
    )(
        pool_in, doc_ids, routes.T, route_weight.T, pool_map, pool_scale[None],
        first_gain[None], first_bias[None], second_gain[None], second_bias[None], *loaded,
    )


def solution(mesh):
    return jax.shard_map(
        functools.partial(body, mesh.shape["sp"], mesh.shape["tp"]),
        mesh=mesh,
        in_specs=(
            P("tp", "sp"),
            P("sp"),
            P(),
            P(),
            P(None, "tp"),
            P("sp", "tp"),
            P("sp", "tp"),
            P("tp"),
            P("tp"),
            P("sp", None),
            P("sp", None),
            P("sp", None, "tp"),
            P("sp", None, "tp"),
            P("sp", None, "tp"),
            P("tp"),
            P("tp"),
        ),
        out_specs=P("sp", "tp"),
        check_vma=False,
    )
```

```python
import functools

import jax
import jax.numpy as jnp
from jax import lax
from jax.experimental import pallas as pl
from jax.experimental.pallas import tpu as pltpu
from jax.sharding import PartitionSpec as P

GROUP_W = 64


EPS = 1e-05
ALPHA = 8.0**0.25
halo_len = 16


def shifted(shard, axis, by):
    size = lax.axis_size(axis)
    pairs = [(i, i + by) for i in range(size) if 0 <= i + by < size]
    return lax.ppermute(shard, axis, pairs)


def entering(shard, axis, combine, identity):
    size, place = (lax.axis_size(axis), lax.axis_index(axis))
    everything = jax.tree.map(lambda part: lax.all_gather(part, axis), shard)
    start = jax.tree.map(
        lambda part, zero: jnp.broadcast_to(jnp.asarray(zero, part.dtype), part.shape),
        shard,
        identity,
    )

    def turn(k, before):
        reached = k < place
        new = combine(before, jax.tree.map(lambda part: part[k], everything))
        return jax.tree.map(lambda a, b: jnp.where(reached, a, b), new, before)

    return lax.fori_loop(0, size, turn, start)


def carry_join(earlier, later):
    keeping = 1.0 - later[2]
    return (
        later[0] + keeping * earlier[0],
        later[1] + keeping * earlier[1],
        jnp.maximum(earlier[2], later[2]),
    )


def apply_norm(row_data, totals, gain_vec, bias_vec, features):
    row_mean = totals[0][:, None] / features
    row_var = totals[1][:, None] / features - row_mean * row_mean
    return (row_data - row_mean) * lax.rsqrt(row_var + EPS) * gain_vec + bias_vec


def pool_scales(pool_in, doc_ids):
    channels_dev, positions = pool_in.shape
    edge_block = jnp.concatenate(
        [
            pool_in[:, positions - halo_len :],
            doc_ids[None, positions - halo_len :].astype(jnp.bfloat16),
        ],
        axis=0,
    )
    previous = shifted(edge_block, "sp", 1)
    prior_ids = jnp.where(
        lax.axis_index("sp") == 0, -1.0, previous[channels_dev].astype(jnp.float32)
    )
    ids_ext = jnp.concatenate([prior_ids, doc_ids.astype(jnp.float32)])
    inputs_ext = jnp.concatenate([previous[:channels_dev], pool_in], axis=1).astype(jnp.float32)
    length = positions + halo_len
    opening = jnp.concatenate([jnp.zeros((1,), bool), ids_ext[1:] != ids_ext[:-1]])
    places = jnp.arange(length, dtype=jnp.int32)
    doc_start = lax.cummax(jnp.where(opening, places, 0), axis=0)
    prefix = jnp.concatenate(
        [jnp.zeros((channels_dev, 1), jnp.float32), jnp.cumsum(inputs_ext, axis=1)], axis=1
    )
    start_here = doc_start[halo_len:]
    upper_at = places[halo_len:] + 1
    at_start = jnp.take(prefix, start_here, axis=1)
    current = prefix[:, halo_len + 1 :]
    group_id = (
        lax.axis_index("tp") * channels_dev + jnp.arange(channels_dev, dtype=jnp.int32)
    ) // GROUP_W
    doc_mask = (group_id % 2 == 1)[:, None]
    window = jnp.left_shift(2, group_id // 2 % 4)[:, None]
    lagged = jnp.zeros((channels_dev, positions), jnp.float32)
    for octave in range(4):
        window_len = 2 << octave
        begin = halo_len + 1 - window_len
        lagged = lagged + jnp.where(window == window_len, prefix[:, begin : begin + positions], 0.0)
    lower_at = jnp.maximum(upper_at[None, :] - window, start_here[None, :])
    win_sum = current - jnp.where(
        start_here[None, :] > upper_at[None, :] - window, at_start, lagged
    )
    win_count = (upper_at[None, :] - lower_at).astype(jnp.float32)
    opened = start_here >= halo_len
    local_sum = current - jnp.where(opened[None, :], at_start, prefix[:, halo_len : halo_len + 1])
    local_count = (upper_at - jnp.maximum(start_here, halo_len)).astype(jnp.float32)
    last_start = doc_start[length - 1]
    last_base = jnp.where(
        last_start >= halo_len,
        lax.dynamic_slice_in_dim(prefix, last_start, 1, 1)[:, 0],
        prefix[:, halo_len],
    )
    summary = (
        prefix[:, length] - last_base,
        (length - jnp.maximum(last_start, halo_len)).astype(jnp.float32),
        (last_start >= halo_len).astype(jnp.float32),
    )
    nothing = (jnp.zeros((channels_dev,), jnp.float32), jnp.float32(0.0), jnp.float32(0.0))
    carried = entering(summary, "sp", carry_join, nothing)
    doc_sum = local_sum + jnp.where(opened[None, :], 0.0, carried[0][:, None])
    doc_count = local_count + jnp.where(opened, 0.0, carried[1])
    pooled = (
        jnp.where(doc_mask, doc_sum / doc_count[None, :], win_sum / win_count)
        - inputs_ext[:, halo_len:]
    )
    return pooled.astype(jnp.bfloat16)


def general_body(
    pool_in,
    doc_ids,
    pool_map,
    pool_scale,
    w_out,
    gate_logit,
    residual,
    first_gain,
    first_bias,
    routes,
    route_weight,
    w_gate,
    w_up,
    w_down,
    second_gain,
    second_bias,
):
    pooled = pool_scales(pool_in, doc_ids)
    positions = pool_in.shape[1]
    features = residual.shape[1] * lax.axis_size("tp")
    gathered = lax.all_gather(pooled, "tp", axis=0, tiled=True)
    group_count = gathered.shape[0] // GROUP_W
    grouped = jnp.einsum(
        "gct,gcd->tgd",
        gathered.reshape(group_count, GROUP_W, positions),
        pool_map,
        preferred_element_type=jnp.float32,
    )
    mapped = (grouped.reshape(positions, group_count * GROUP_W) * pool_scale).astype(jnp.bfloat16)
    mixer_out = jnp.dot(mapped, w_out, preferred_element_type=jnp.float32) * jax.nn.sigmoid(
        gate_logit.astype(jnp.float32)
    )
    mixed_rows = ALPHA * residual.astype(jnp.float32) + mixer_out
    first_totals = lax.psum(
        (jnp.sum(mixed_rows, axis=1), jnp.sum(mixed_rows * mixed_rows, axis=1)), "tp"
    )
    normed = apply_norm(mixed_rows, first_totals, first_gain, first_bias, features).astype(
        jnp.bfloat16
    )
    experts = lax.axis_size("sp")
    pairs = routes.shape[1]
    slots_per = 2 * positions * pairs // experts
    flat_routes = routes.reshape(-1)
    one_hot = (flat_routes[:, None] == jnp.arange(experts, dtype=jnp.int32)[None, :]).astype(
        jnp.int32
    )
    slot_rank = jnp.sum((jnp.cumsum(one_hot, axis=0, dtype=jnp.int32) - 1) * one_hot, axis=1)
    slot_ids = flat_routes * slots_per + slot_rank
    token_of = jnp.arange(flat_routes.shape[0], dtype=jnp.int32) // pairs
    outgoing = (
        jnp.zeros((experts * slots_per, normed.shape[1]), jnp.bfloat16)
        .at[slot_ids]
        .set(normed[token_of])
    )
    arrived = lax.all_to_all(outgoing, "sp", split_axis=0, concat_axis=0, tiled=True)
    inputs = lax.all_gather(arrived, "tp", axis=1, tiled=True)
    gate_part = jnp.dot(inputs, w_gate[0], preferred_element_type=jnp.float32)
    up_part = jnp.dot(inputs, w_up[0], preferred_element_type=jnp.float32)
    hidden = (jax.nn.silu(gate_part) * up_part).astype(jnp.bfloat16)
    down_part = w_down[0]
    result = jnp.dot(
        lax.all_gather(hidden, "tp", axis=1, tiled=True),
        down_part,
        preferred_element_type=jnp.float32,
    )
    returned = lax.all_to_all(
        result.astype(jnp.bfloat16), "sp", split_axis=0, concat_axis=0, tiled=True
    )
    picked = returned[slot_ids].astype(jnp.float32).reshape(positions, pairs, returned.shape[1])
    moe_sum = jnp.sum(picked * route_weight[:, :, None], axis=1)
    final_rows = ALPHA * normed.astype(jnp.float32) + moe_sum
    second_totals = lax.psum(
        (jnp.sum(final_rows, axis=1), jnp.sum(final_rows * final_rows, axis=1)), "tp"
    )
    return apply_norm(final_rows, second_totals, second_gain, second_bias, features).astype(
        jnp.bfloat16
    )


NT = (((1,), (1,)), ((), ()))
F32 = jnp.float32
BF16 = jnp.bfloat16
LANES = 128


def dot_nt(a, b):
    return lax.dot_general(a, b, NT, preferred_element_type=F32)


def dot_nn(a, b):
    return jnp.dot(a, b, preferred_element_type=F32)


def layout():
    sp, tp = lax.axis_index("sp"), lax.axis_index("tp")
    plane, core = sp // 2, lax.rem(sp, 2)
    y, x = tp // 2, lax.rem(tp, 2)
    return plane, core, y, x


def near_peers():
    tp = lax.axis_index("tp")
    beside = tp + 1 - 2 * lax.rem(tp, 2)
    return beside, lax.rem(tp + 2, 4), lax.rem(beside + 2, 4)


def greet(n_sp):
    sp = lax.axis_index("sp")
    beside, below, far = near_peers()
    barrier = pltpu.get_barrier_semaphore()
    for d in range(n_sp):
        if d:
            pl.semaphore_signal(barrier, inc=1, device_id={"sp": lax.rem(sp + d, n_sp)})
        pl.semaphore_signal(
            barrier, inc=1, device_id={"sp": lax.rem(sp + d, n_sp), "tp": beside}
        )
    for peer in (below, far):
        pl.semaphore_signal(barrier, inc=1, device_id={"tp": peer})


def all_here(n_sp):
    pl.semaphore_wait(pltpu.get_barrier_semaphore(), 2 * n_sp + 1)


def remote_to(src, dst, send, recv, device):
    return pltpu.make_async_remote_copy(
        src_ref=src, dst_ref=dst, send_sem=send, recv_sem=recv, device_id=device
    )


def remote(src, dst, send, recv, axis, peer):
    return remote_to(src, dst, send, recv, {axis: peer})


def share(buf, axis, n, send, recv):
    me = lax.axis_index(axis)
    for d in range(1, n):
        remote(
            buf.at[me], buf.at[me], send.at[d], recv.at[me], axis, lax.rem(me + d, n)
        ).start()


def collect(buf, axis, n, send, recv):
    me = lax.axis_index(axis)
    for d in range(1, n):
        other = lax.rem(me + d, n)
        remote(buf.at[other], buf.at[other], send.at[d], recv.at[other], axis, other).wait_recv()


def settle(buf, axis, n, send, recv):
    me = lax.axis_index(axis)
    for d in range(1, n):
        remote(
            buf.at[me], buf.at[me], send.at[d], recv.at[me], axis, lax.rem(me + d, n)
        ).wait_send()


def row_totals(rows, stats, n_tp, send, recv, between=None):
    me = lax.axis_index("tp")
    lane = lax.broadcasted_iota(jnp.int32, (rows.shape[0], LANES), 1)
    first = jnp.sum(rows, axis=1, keepdims=True)
    second = jnp.sum(rows * rows, axis=1, keepdims=True)
    both = jnp.where(lane == 0, first, jnp.where(lane == 1, second, 0.0))
    stats[me] = jnp.transpose(both)[:8]
    share(stats, "tp", n_tp, send, recv)
    if between is not None:
        between()
    collect(stats, "tp", n_tp, send, recv)
    total = stats[0]
    for k in range(1, n_tp):
        total = total + stats[k]
    total = jnp.concatenate([total, jnp.zeros((LANES - 8, total.shape[1]), F32)], axis=0)
    columns = jnp.transpose(total)
    return columns[:, 0:1], columns[:, 1:2]


def normalise(rows, totals, gain, bias, features):
    mean = totals[0] / features
    var = totals[1] / features - mean * mean
    return (rows - mean) * lax.rsqrt(var + EPS) * gain + bias


def layer_kernel(
    n_sp, n_tp, pool, doc_ids, route_row, weight_row, pool_map, scale, gain, bias, gain2, bias2,
    w_out_hbm, gate_hbm, residual_hbm, w_gate_hbm, w_up_hbm, w_down_hbm, out,
    w_out, gate, residual, w_gate, w_up, w_down,
    doc_row, halo, halo_ids, tails, mapped, stats, stats2, tables, blocks,
    aside, passing, inputs, hidden, result, back, load_sem, w_send, w_recv,
    halo_send, halo_recv, tail_send, tail_recv, map_send, map_recv, stat_send, stat_recv,
    t_send, t_recv, z_send, z_recv, a_send, a_recv, p_send, p_recv, y_send, y_recv, d_send, d_recv,
    h_send, h_recv, r_send, r_recv, stat2_send, stat2_recv,
):
    sp, tp = lax.axis_index("sp"), lax.axis_index("tp")
    plane, core, y, x = layout()
    partner = sp + 1 - 2 * core
    beside, below, far = near_peers()
    n_z = n_sp // 2
    steps = 2 * n_z
    channels, positions = pool.shape
    part = residual.shape[1]
    half = aside.shape[1]
    slots = 2 * half
    features = part * n_tp
    toward = 1 - 2 * (plane // (n_z // 2))
    straight = x == core
    shift = jnp.where((plane > 0) & (plane < n_z - 1), 1, 0)
    expert = 2 * plane + x
    loads = [
        pltpu.make_async_copy(src, dst, load_sem.at[i])
        for i, (src, dst) in enumerate([
            (w_out_hbm, w_out), (gate_hbm, gate), (residual_hbm, residual),
        ])
    ]
    for load in loads:
        load.start()
    pieces = []
    for pair, cuts in ((((w_gate_hbm, w_gate), (w_up_hbm, w_up)), 8), (((w_down_hbm, w_down),), 8)):
        for cut in range(cuts):
            for src, dst in pair:
                size = dst.shape[0] // cuts
                span = pl.ds(cut * size, size)
                pieces.append((src.at[span], dst.at[span]))
    crossing = [
        remote_to(
            src, dst, w_send.at[i], w_recv.at[i],
            {"sp": 2 * plane + x, "tp": 2 * y + core},
        )
        for i, (src, dst) in enumerate(pieces)
    ]
    staying = [
        pltpu.make_async_copy(src, dst, w_recv.at[i]) for i, (src, dst) in enumerate(pieces)
    ]

    @pl.when(straight)
    def _():
        for copy in staying:
            copy.start()

    def cross(first, last):
        @pl.when(jnp.logical_not(straight))
        def _():
            for copy in crossing[first:last]:
                copy.start()

    def weights_here(first, last):
        @pl.when(straight)
        def _():
            for copy in staying[first:last]:
                copy.wait()

        @pl.when(jnp.logical_not(straight))
        def _():
            for copy in crossing[first:last]:
                copy.wait_recv()

    greet(n_sp)
    doc_row[...] = doc_ids[...].reshape(1, positions)
    ids = doc_row[...].astype(F32)
    in_last = (ids == ids[:, positions - 1 :]).astype(F32)
    tail = dot_nt(jnp.broadcast_to(in_last, (8, positions)).astype(BF16), pool[...])
    kind = lax.broadcasted_iota(jnp.int32, tail.shape, 0)
    tail = jnp.where(kind == 1, jnp.sum(in_last, axis=1, keepdims=True), tail)
    tails[sp] = jnp.where(kind == 2, ids[:, positions - 1 :], tail)
    kind = lax.broadcasted_iota(jnp.int32, (LANES, positions), 0)
    later = lax.broadcasted_iota(jnp.int32, (positions, positions), 1)
    earlier = lax.broadcasted_iota(jnp.int32, (positions, positions), 0)
    ahead = (earlier < later).astype(F32).astype(BF16)
    r0, r1 = route_row[0:1], route_row[1:2]
    named = ((r0 == kind) | (r1 == kind)).astype(F32).astype(BF16)
    rank = dot_nn(named, ahead) + (kind * slots).astype(F32)
    slot0 = jnp.sum(jnp.where(r0 == kind, rank, 0.0), axis=0, keepdims=True)
    slot1 = jnp.sum(jnp.where(r1 == kind, rank, 0.0), axis=0, keepdims=True)
    table = jnp.where(kind == 0, slot0, jnp.where(kind == 1, slot1, 0.0))
    for i, row in enumerate((ids, weight_row[0:1], weight_row[1:2])):
        table = jnp.where(kind == i + 2, row, table)
    tables[plane] = table[:8]

    def table_copy(d):
        to = lax.rem(plane + d, n_z)
        return remote(
            tables.at[plane], tables.at[plane], t_send.at[d], t_recv.at[plane], "sp", 2 * to + core
        )

    columns = jnp.transpose(table)
    col = columns[:, 2:3]
    place = lax.broadcasted_iota(jnp.int32, (positions, LANES + positions), 1) - LANES
    delta = lax.broadcasted_iota(jnp.int32, (positions, LANES + positions), 0) - place
    all_here(n_sp)
    after = lax.rem(sp + 1, n_sp)
    last = pl.ds(positions - LANES, LANES)
    edge = remote(pool.at[:, last], halo, halo_send.at[0], halo_recv.at[0], "sp", after)
    edge_ids = remote(doc_row.at[:, last], halo_ids, halo_send.at[1], halo_recv.at[1], "sp", after)
    edge.start()
    edge_ids.start()
    share(tails, "sp", n_sp, tail_send, tail_recv)
    cross(0, 5)
    for d in range(1, n_z):
        table_copy(d).start()
    edge.wait_recv()
    edge_ids.wait_recv()
    ext = jnp.concatenate([halo[...], pool[...]], axis=1)
    before = jnp.where(sp == 0, -1.0, halo_ids[...].astype(F32))
    ext_ids = jnp.concatenate([before, ids], axis=1)
    together = (col == ext_ids) & (delta >= 0)
    own = (delta == 0).astype(F32).astype(BF16)
    values = dot_nt(own, ext)
    sums, counts, wholes = [], [], []
    per = channels // GROUP_W
    for i in range(per):
        group = tp * per + i
        whole = lax.rem(group, 2) == 1
        window = jnp.left_shift(2, lax.rem(group // 2, 4))
        reach = jnp.where(whole, positions, window)
        least = jnp.where(whole, 0, -LANES)
        mask = (together & (delta < reach) & (place >= least)).astype(F32)
        sums.append(dot_nt(mask.astype(BF16), ext[i * GROUP_W : (i + 1) * GROUP_W]))
        counts.append(jnp.sum(mask, axis=1, keepdims=True))
        wholes.append(whole)
    collect(tails, "sp", n_sp, tail_send, tail_recv)
    opening = col[0:1]
    carry = jnp.zeros((1, channels), F32)
    carry_count = jnp.zeros((1, channels), F32)
    for k in range(n_sp - 1):
        block = tails[k]
        joins = (block[2:3] == opening) & (k < sp)
        carry = carry + jnp.where(joins, block[0:1], 0.0)
        carry_count = carry_count + jnp.where(joins, block[1:2], 0.0)
    goes_on = (col == opening).astype(F32)
    for i in range(per):
        group = tp * per + i
        span = slice(i * GROUP_W, (i + 1) * GROUP_W)
        joined = jnp.where(wholes[i], goes_on, 0.0)
        total = sums[i] + joined * carry[:, span]
        count = counts[i] + joined * carry_count[:, span]
        pooled = (total / count - values[:, span]).astype(BF16)
        factor = scale[:, pl.ds(pl.multiple_of(tp * channels, LANES), channels)][:, span]
        mapped[tp, :, span] = (dot_nn(pooled, pool_map[group]) * factor).astype(BF16)
    share(mapped, "tp", n_tp, map_send, map_recv)
    cross(5, 7)
    for load in loads:
        load.wait()
    opened = jax.nn.sigmoid(gate[...].astype(F32))
    kept = ALPHA * residual[...].astype(F32)
    collect(mapped, "tp", n_tp, map_send, map_recv)
    every = jnp.concatenate([mapped[k] for k in range(n_tp)], axis=1)
    rows = kept + dot_nn(every, w_out[...]) * opened
    totals = row_totals(rows, stats, n_tp, stat_send, stat_recv, lambda: cross(7, 11))
    blocks[plane] = normalise(rows, totals, gain[...], bias[...], features).astype(BF16)

    def unit_plane(m):
        return lax.rem(plane + toward * (m + shift) + 2 * n_z, n_z)

    def packed_unit(p):
        return lax.rem(p - shift + n_z, n_z)

    def hop(u, to, slot):
        return remote(
            blocks.at[u], blocks.at[u], z_send.at[slot], z_recv.at[u], "sp", 2 * to + core
        )

    def z_round(d):
        left, right = plane - d, plane + d

        @pl.when(left >= 0)
        def _():
            hop(left, plane, left).wait_recv()

            @pl.when(plane < n_z - 1)
            def _():
                hop(left, plane + 1, left).start()

        @pl.when(right < n_z)
        def _():
            hop(right, plane, right).wait_recv()

            @pl.when(plane > 0)
            def _():
                hop(right, plane - 1, right).start()

    def aside_copy(i):
        return remote(
            aside.at[i], inputs.at[i, core, tp], a_send.at[i], a_recv.at[i], "tp", beside
        )

    def aside_over(i):
        return remote(aside.at[i], passing.at[i], a_send.at[i], p_recv.at[i], "sp", partner)

    def aside_pass(i):
        return remote_to(
            passing.at[i], inputs.at[i, 1 - core, tp], p_send.at[i], a_recv.at[i],
            {"sp": partner, "tp": beside},
        )

    def down_y(i, k, which):
        ref = inputs.at[i, core, which]
        return remote(ref, ref, y_send.at[i, k], y_recv.at[i, k], "tp", below)

    def over(i, k, which, owner):
        ref = inputs.at[i, owner, which]
        return remote(ref, ref, d_send.at[i, k], d_recv.at[i, k], "sp", partner)

    def pack(m):
        u = unit_plane(m)
        slot_rows = tables[u]
        line = lax.broadcasted_iota(jnp.int32, (slots, positions), 0)

        def pick(e):
            mine = (line + e * slots).astype(F32)
            hit = (mine == slot_rows[0:1]) | (mine == slot_rows[1:2])
            return dot_nn(hit.astype(F32).astype(BF16), blocks[u]).astype(BF16)

        away = pick(2 * plane + 1 - x)
        for h in range(2):
            aside[2 * m + h] = away[h * half : (h + 1) * half]
            i = 2 * m + h

            @pl.when(straight)
            def _():
                aside_copy(i).start()

            @pl.when(jnp.logical_not(straight))
            def _():
                aside_over(i).start()

        kept_rows = pick(expert)
        for h in range(2):
            i = 2 * m + h
            inputs[i, core, tp] = kept_rows[h * half : (h + 1) * half]
            down_y(i, 0, tp).start()
            over(i, 0, tp, core).start()

        @pl.when(straight)
        def _():
            for h in range(2):
                aside_over(2 * m + h).wait_recv()
                aside_pass(2 * m + h).start()

    def beside_arrived(i):
        remote(
            aside.at[i], inputs.at[i, core, beside], a_send.at[i], a_recv.at[i], "tp", beside
        ).wait_recv()
        down_y(i, 1, beside).start()
        over(i, 1, beside, core).start()

    def below_arrived(i):
        for k, which in enumerate((below, far)):
            down_y(i, k, which).wait_recv()
            over(i, 2 + k, which, core).start()

    quarter = 2 * y + core

    def hidden_over(i, k, q):
        ref = hidden.at[i, q]
        return remote(ref, ref, h_send.at[i, k], h_recv.at[i, k], "sp", partner)

    def hidden_down(i, q):
        ref = hidden.at[i, q]
        return remote(ref, ref, h_send.at[i, 1], h_recv.at[i, 1], "tp", below)

    def expand(i):
        for k, which in enumerate((tp, beside, below, far)):
            over(i, k, which, 1 - core).wait_recv()
        rows = jnp.concatenate(
            [inputs[i, :, k].reshape(slots, part) for k in range(n_tp)], axis=1
        )
        gated = dot_nn(rows, w_gate[...])
        up = dot_nn(rows, w_up[...])
        hidden[i, quarter] = (gated * jax.nn.sigmoid(gated) * up).astype(BF16)
        hidden_down(i, quarter).start()
        hidden_over(i, 0, quarter).start()

    q_partner = 2 * y + 1 - core
    q_below = 2 * (1 - y) + core
    q_far = 2 * (1 - y) + 1 - core

    def is_own(i, c):
        return (unit_plane(i // 2) == plane) & straight & (core == c)

    def result_copy(i, c):
        u = unit_plane(i // 2)
        return remote_to(
            result.at[i, c], back.at[expert, lax.rem(i, 2)], r_send.at[i, c],
            r_recv.at[expert, lax.rem(i, 2)], {"sp": 2 * u + c, "tp": 2 * y + core},
        )

    def below_hidden(i):
        hidden_down(i, q_below).wait_recv()
        hidden_over(i, 2, q_below).start()

    def contract(i):
        hidden_over(i, 0, q_partner).wait_recv()
        hidden_over(i, 2, q_far).wait_recv()
        rows = jnp.concatenate([hidden[i, k] for k in range(n_tp)], axis=1)
        block = dot_nn(rows, w_down[...]).astype(BF16)
        for c in range(2):
            result[i, c] = block[c * half : (c + 1) * half]

            @pl.when(jnp.logical_not(is_own(i, c)))
            def _():
                result_copy(i, c).start()

            @pl.when(is_own(i, c))
            def _():
                back[expert, lax.rem(i, 2)] = block[c * half : (c + 1) * half]

    @pl.when(plane < n_z - 1)
    def _():
        hop(plane, plane + 1, plane).start()

    @pl.when(plane > 0)
    def _():
        hop(plane, plane - 1, n_z).start()

    pack(packed_unit(0))
    cross(11, 16)
    for d in range(1, n_z):
        other = lax.rem(plane + d, n_z)
        remote(
            tables.at[other], tables.at[other], t_send.at[d], t_recv.at[other], "sp", partner
        ).wait_recv()

    def both_beside(p):
        i = 2 * packed_unit(p)
        beside_arrived(i)
        beside_arrived(i + 1)

    both_beside(0)
    z_round(1)
    pack(packed_unit(1))
    cross(16, 20)

    def step(p, _):
        @pl.when(p + 1 < n_z)
        def _():
            both_beside(p + 1)

        @pl.when(p + 2 < n_z)
        def _():
            z_round(p + 2)
            pack(packed_unit(p + 2))

        @pl.when(p == 0)
        def _():
            cross(20, 24)

        @pl.when(p == 1)
        def _():
            cross(24, 24)

        @pl.when(p > 0)
        def _():
            below_hidden(2 * p - 2)

        @pl.when(p > 0)
        def _():
            below_hidden(2 * p - 1)

        @pl.when(p == 1)
        def _():
            weights_here(16, 24)

        @pl.when(p > 0)
        def _():
            contract(2 * p - 2)

        @pl.when(p > 0)
        def _():
            contract(2 * p - 1)

        @pl.when(p == 0)
        def _():
            weights_here(0, 16)

        @pl.when(p < n_z)
        def _():
            below_arrived(2 * p + 0)
            expand(2 * p + 0)

        @pl.when(p < n_z)
        def _():
            below_arrived(2 * p + 1)
            expand(2 * p + 1)

        return 0

    lax.fori_loop(0, n_z + 1, step, 0)
    at0, at1 = columns[:, 0:1], columns[:, 1:2]
    spot = lax.broadcasted_iota(jnp.int32, (positions, 2 * slots), 1)
    sum0 = jnp.zeros((positions, part), F32)
    sum1 = jnp.zeros((positions, part), F32)
    inner = jnp.where((plane > 0) & (plane < n_z - 1), 1, 0)
    for d in range(n_z):
        u = lax.rem(plane + toward * (d + inner) + 2 * n_z, n_z)
        for side in range(2):
            e = 2 * u + side
            local = (u == plane) & straight & (x == side)

            @pl.when(jnp.logical_not(local))
            def _():
                for h in range(2):
                    remote(
                        result.at[0, 0], back.at[e, h], r_send.at[0, 0], r_recv.at[e, h],
                        "sp", partner,
                    ).wait_recv()

        returned = back[pl.ds(2 * u, 2)].reshape(2 * slots, part)
        spots = (spot + 2 * slots * u).astype(F32)
        sum0 = sum0 + dot_nn((spots == at0).astype(F32).astype(BF16), returned)
        sum1 = sum1 + dot_nn((spots == at1).astype(F32).astype(BF16), returned)
    moe = columns[:, 3:4] * sum0 + columns[:, 4:5] * sum1
    rows = ALPHA * blocks[plane].astype(F32) + moe
    totals = row_totals(rows, stats2, n_tp, stat2_send, stat2_recv)
    out[...] = normalise(rows, totals, gain2[...], bias2[...], features).astype(BF16)

    def drain(i, _):
        aside_copy(i).wait_send()

        @pl.when(straight)
        def _():
            aside_pass(i).wait_send()

        for k, which in enumerate((tp, beside)):
            down_y(i, k, which).wait_send()
        for k, which in enumerate((tp, beside, below, far)):
            over(i, k, which, core).wait_send()
        hidden_down(i, quarter).wait_send()
        hidden_over(i, 0, quarter).wait_send()
        hidden_over(i, 2, q_below).wait_send()
        for c in range(2):
            @pl.when(jnp.logical_not(is_own(i, c)))
            def _():
                result_copy(i, c).wait_send()

        return 0

    lax.fori_loop(0, steps, drain, 0)

    @pl.when(jnp.logical_not(straight))
    def _():
        for copy in crossing:
            copy.wait_send()

    @pl.when(plane < n_z - 1)
    def _():
        hop(plane, plane + 1, plane).wait_send()
        for d in range(1, n_z - 1):
            @pl.when(plane - d >= 0)
            def _():
                hop(plane - d, plane + 1, plane - d).wait_send()

    @pl.when(plane > 0)
    def _():
        hop(plane, plane - 1, n_z).wait_send()
        for d in range(1, n_z - 1):
            @pl.when(plane + d < n_z)
            def _():
                hop(plane + d, plane - 1, plane + d).wait_send()

    for d in range(1, n_z):
        table_copy(d).wait_send()
    edge.wait_send()
    edge_ids.wait_send()
    settle(tails, "sp", n_sp, tail_send, tail_recv)
    settle(mapped, "tp", n_tp, map_send, map_recv)
    settle(stats, "tp", n_tp, stat_send, stat_recv)
    settle(stats2, "tp", n_tp, stat2_send, stat2_recv)


def body(n_sp, n_tp, *args):
    (pool_in, doc_ids, pool_map, pool_scale, w_out, gate_logit, residual, first_gain, first_bias,
     routes, route_weight, w_gate, w_up, w_down, second_gain, second_bias) = args
    channels, positions = pool_in.shape
    part = residual.shape[1]
    pairs = routes.shape[1]
    slots = 2 * positions * pairs // n_sp
    units = w_gate.shape[2]
    small = n_sp == 8 and n_tp == 4 and pairs == 2 and slots % 32 == 0
    if not small or channels % LANES or positions % LANES or part % LANES or units % LANES:
        return general_body(*args)
    dma = pltpu.SemaphoreType.DMA
    n_z = n_sp // 2
    steps = 2 * n_z
    half = slots // 2
    loaded = (w_out, gate_logit, residual, w_gate[0], w_up[0], w_down[0])
    vmem = pl.BlockSpec(memory_space=pltpu.VMEM)
    any_space = pl.BlockSpec(memory_space=pl.ANY)
    return pl.pallas_call(
        functools.partial(layer_kernel, n_sp, n_tp),
        out_shape=jax.ShapeDtypeStruct(residual.shape, BF16),
        in_specs=[vmem] * 10 + [any_space] * len(loaded),
        out_specs=vmem,
        scratch_shapes=[
            *(pltpu.VMEM(x.shape, x.dtype) for x in loaded),
            pltpu.VMEM((1, positions), jnp.int32),
            pltpu.VMEM((channels, LANES), BF16),
            pltpu.VMEM((1, LANES), jnp.int32),
            pltpu.VMEM((n_sp, 8, channels), F32),
            pltpu.VMEM((n_tp, positions, channels), BF16),
            pltpu.VMEM((n_tp, 8, positions), F32),
            pltpu.VMEM((n_tp, 8, positions), F32),
            pltpu.VMEM((n_z, 8, positions), F32),
            pltpu.VMEM((n_z, positions, part), BF16),
            pltpu.VMEM((steps, half, part), BF16),
            pltpu.VMEM((steps, half, part), BF16),
            pltpu.VMEM((steps, 2, n_tp, half, part), BF16),
            pltpu.VMEM((steps, n_tp, slots, units), BF16),
            pltpu.VMEM((steps, 2, half, part), BF16),
            pltpu.VMEM((n_sp, 2, half, part), BF16),
            dma((3,)), dma((24,)), dma((24,)),
            dma((2,)), dma((2,)), dma((n_sp,)), dma((n_sp,)),
            dma((n_tp,)), dma((n_tp,)), dma((n_tp,)), dma((n_tp,)),
            dma((n_z,)), dma((n_z,)), dma((n_z + 1,)), dma((n_z,)),
            dma((steps,)), dma((steps,)), dma((steps,)), dma((steps,)), dma((steps, 2)), dma((steps, 2)),
            dma((steps, 4)), dma((steps, 4)), dma((steps, 3)), dma((steps, 3)),
            dma((steps, 2)), dma((n_sp, 2)),
            dma((n_tp,)), dma((n_tp,)),
        ],
        compiler_params=pltpu.CompilerParams(
            collective_id=0, has_side_effects=True, vmem_limit_bytes=60 << 20
        ),
    )(
        pool_in, doc_ids, routes.T, route_weight.T, pool_map, pool_scale[None],
        first_gain[None], first_bias[None], second_gain[None], second_bias[None], *loaded,
    )


def solution(mesh):
    return jax.shard_map(
        functools.partial(body, mesh.shape["sp"], mesh.shape["tp"]),
        mesh=mesh,
        in_specs=(
            P("tp", "sp"),
            P("sp"),
            P(),
            P(),
            P(None, "tp"),
            P("sp", "tp"),
            P("sp", "tp"),
            P("tp"),
            P("tp"),
            P("sp", None),
            P("sp", None),
            P("sp", None, "tp"),
            P("sp", None, "tp"),
            P("sp", None, "tp"),
            P("tp"),
            P("tp"),
        ),
        out_specs=P("sp", "tp"),
        check_vma=False,
    )
```
